128 devices in a mesh: fs: 16 (over z, x), tp: 8 (over y, core).
Axes of the slice: x: 4, y: 4, z: 4, core: 2. Of those that a mesh axis runs over, the one named last changes fastest.
Arguments:
- mixer_input: bfloat16 [16384, 4096], P('fs'), may hold values from -6 to 6
- cell_output: bfloat16 [16384, 2048], P('fs'), may hold values from -6 to 6
- query_grad: bfloat16 [16384, 2048], P('fs', 'tp'), may hold values from -4 to 4
- value_grad: bfloat16 [16384, 2048], P('fs', 'tp'), may hold values from -4 to 4
- output_grad: bfloat16 [16384, 4096], P('fs', 'tp'), may hold values from -4 to 4
- query_weight: float32 [4096, 2048], P('fs', 'tp'), may hold values from -6 to 6
- value_weight: float32 [4096, 2048], P('fs', 'tp'), may hold values from -6 to 6
- output_weight: float32 [2048, 4096], P('fs', 'tp'), may hold values from -6 to 6
- query_basis: bfloat16 [4096, 128], P('fs'), may hold values from -0.09375 to 0.09375
- value_basis: bfloat16 [4096, 128], P('fs'), may hold values from -0.09375 to 0.09375
- output_basis: bfloat16 [2048, 128], P('fs'), may hold values from -0.125 to 0.125
- query_mean: float32 [128, 2048], P(None, 'tp'), may hold values from -6 to 6
- value_mean: float32 [128, 2048], P(None, 'tp'), may hold values from -6 to 6
- output_mean: float32 [128, 4096], P(None, 'tp'), may hold values from -6 to 6
- query_square: float32 [128, 2048], P(None, 'tp'), may hold values from 0.25 to 4
- value_square: float32 [128, 2048], P(None, 'tp'), may hold values from 0.25 to 4
- output_square: float32 [128, 4096], P(None, 'tp'), may hold values from 0.25 to 4
Outputs:
- query_step: float32 [4096, 2048], P('fs', 'tp')
- value_step: float32 [4096, 2048], P('fs', 'tp')
- output_step: float32 [2048, 4096], P('fs', 'tp')
- query_copy: bfloat16 [4096, 2048], P(None, 'tp')
- value_copy: bfloat16 [4096, 2048], P(None, 'tp')
- output_copy: bfloat16 [2048, 4096], P(None, 'tp')
- query_first: float32 [128, 2048], P(None, 'tp')
- value_first: float32 [128, 2048], P(None, 'tp')
- output_first: float32 [128, 4096], P(None, 'tp')
- query_second: float32 [128, 2048], P(None, 'tp')
- value_second: float32 [128, 2048], P(None, 'tp')
- output_second: float32 [128, 4096], P(None, 'tp')
The draws below stay inside these ranges and needn't reach their ends.
All inputs are finite; a program needn't handle non-finite values.
Results may differ from the reference program's by a relative error of at most 0.013.
Values may be sent and summed in bfloat16 or wider, within the bound.
A program may use at most 128 MiB of HBM per device.

```python
import math
import jax
import jax.numpy as jnp
from jax import lax

MODEL = 4096
CELL = 2048
RANK = 128
TOKENS = 16384


def input_rows(key):
    return jnp.clip(jax.random.normal(jax.random.fold_in(key, 101), (TOKENS, MODEL), jnp.float32), -6.0, 6.0)


def readout_rows(key):
    return jnp.clip(jax.random.normal(jax.random.fold_in(key, 102), (TOKENS, CELL), jnp.float32), -6.0, 6.0)


def coherent_grad(key, rows, salt, width):
    inner = rows.shape[1]
    noise = jnp.clip(jax.random.normal(jax.random.fold_in(key, salt), (TOKENS, width), jnp.float32), -6.0, 6.0) * (1.0 / math.sqrt(TOKENS))
    heading = jax.random.normal(jax.random.fold_in(key, salt + 1), (inner,), jnp.float32) * (1.0 / math.sqrt(inner))
    column = jnp.clip(jax.random.normal(jax.random.fold_in(key, salt + 2), (width,), jnp.float32), -3.0, 3.0)
    strength = 4.0 * math.sqrt(inner) / TOKENS
    along = jnp.dot(rows, heading, precision=lax.Precision.HIGHEST)
    return jnp.clip(noise + strength * along[:, None] * column[None, :], -4.0, 4.0)


def draw_mixer_input(key, part):
    return input_rows(key).astype(jnp.bfloat16)


def draw_cell_output(key, part):
    return readout_rows(key).astype(jnp.bfloat16)


def draw_query_grad(key, part):
    return coherent_grad(key, input_rows(key), 201, CELL).astype(jnp.bfloat16)


def draw_value_grad(key, part):
    return coherent_grad(key, input_rows(key), 211, CELL).astype(jnp.bfloat16)


def draw_output_grad(key, part):
    return coherent_grad(key, readout_rows(key), 221, MODEL).astype(jnp.bfloat16)


def shard_levels(key, dims, pieces, low, high):
    level, own = 1.0, jax.random.fold_in(key, 6)
    for axis_at, blocks in pieces:
        heights = jnp.exp(jax.random.uniform(jax.random.fold_in(own, axis_at), (blocks,), jnp.float32, low / len(pieces), high / len(pieces)))
        level = level * jnp.repeat(heights, dims[axis_at] // blocks).reshape([-1 if axis == axis_at else 1 for axis in range(len(dims))])
    return level


def gaussian(own_key, extent, deviation, reach, cuts=(), kind=jnp.bfloat16):
    array = deviation * jax.random.normal(own_key, extent, jnp.float32)
    if cuts:
        array = array * shard_levels(own_key, extent, cuts, -0.22, 0.18)
    return jnp.clip(array, -reach, reach).astype(kind)


def setup_inputs(seed: int = 0) -> dict:
    seeds = jax.random.split(jax.random.key(seed), 18)
    return {
        "mixer_input": draw_mixer_input(jax.random.fold_in(seeds[17], 71), 0),
        "cell_output": draw_cell_output(jax.random.fold_in(seeds[17], 71), 0),
        "query_grad": draw_query_grad(jax.random.fold_in(seeds[17], 71), 0),
        "value_grad": draw_value_grad(jax.random.fold_in(seeds[17], 71), 0),
        "output_grad": draw_output_grad(jax.random.fold_in(seeds[17], 71), 0),
        "query_weight": gaussian(seeds[5], (MODEL, CELL), 1.0, 6.0, ((0, 16), (1, 8)), jnp.float32),
        "value_weight": gaussian(seeds[6], (MODEL, CELL), 1.0, 6.0, ((0, 16), (1, 8)), jnp.float32),
        "output_weight": gaussian(seeds[7], (CELL, MODEL), 1.0, 6.0, ((0, 16), (1, 8)), jnp.float32),
        "query_basis": gaussian(seeds[8], (MODEL, RANK), MODEL ** -0.5, 0.09375, ((0, 16),)),
        "value_basis": gaussian(seeds[9], (MODEL, RANK), MODEL ** -0.5, 0.09375, ((0, 16),)),
        "output_basis": gaussian(seeds[10], (CELL, RANK), CELL ** -0.5, 0.125, ((0, 16),)),
        "query_mean": gaussian(seeds[11], (RANK, CELL), 1.0, 6.0, ((1, 8),), jnp.float32),
        "value_mean": gaussian(seeds[12], (RANK, CELL), 1.0, 6.0, ((1, 8),), jnp.float32),
        "output_mean": gaussian(seeds[13], (RANK, MODEL), 1.0, 6.0, ((1, 8),), jnp.float32),
        "query_square": jnp.clip(jnp.exp(math.log(4.0) - 2.7725887 * jax.random.uniform(seeds[14], (RANK, CELL), jnp.float32) ** shard_levels(seeds[14], (RANK, CELL), ((1, 8),), -0.2, 0.2)), 0.25, 4.0),
        "value_square": jnp.clip(jnp.exp(math.log(4.0) - 2.7725887 * jax.random.uniform(seeds[15], (RANK, CELL), jnp.float32) ** shard_levels(seeds[15], (RANK, CELL), ((1, 8),), -0.2, 0.2)), 0.25, 4.0),
        "output_square": jnp.clip(jnp.exp(math.log(4.0) - 2.7725887 * jax.random.uniform(seeds[16], (RANK, MODEL), jnp.float32) ** shard_levels(seeds[16], (RANK, MODEL), ((1, 8),), -0.2, 0.2)), 0.25, 4.0),
    }


beta_first = 0.8
beta_second = 0.9
floor_mean = 0.005
learn_rate = 0.05

def across(leading, trailing):
    return lax.dot_general(leading, trailing, (((0,), (0,)), ((), ())), preferred_element_type=jnp.float32)

def moments(gradient, basis, mean_old, square_old):
    factor_full = basis.astype(jnp.float32)
    projected = lax.dot_general(factor_full, gradient, (((0,), (0,)), ((), ())), precision=lax.Precision.HIGHEST, preferred_element_type=jnp.float32)
    moment_one = beta_first * mean_old + (1.0 - beta_first) * projected
    moment_two = beta_second * square_old + (1.0 - beta_second) * projected * projected
    direction = moment_one / jnp.sqrt(moment_two)
    lowrank = jnp.dot(factor_full, direction, precision=lax.Precision.HIGHEST, preferred_element_type=jnp.float32)
    return (lowrank, moment_one, moment_two)

def reference(mixer_input, cell_output, query_grad, value_grad, output_grad, query_weight, value_weight, output_weight, query_basis, value_basis, output_basis, query_mean, value_mean, output_mean, query_square, value_square, output_square):
    gradient_query = across(mixer_input, query_grad)
    gradient_value = across(mixer_input, value_grad)
    gradient_output = across(cell_output, output_grad)
    low_query, query_first, query_second = moments(gradient_query, query_basis, query_mean, query_square)
    low_value, value_first, value_second = moments(gradient_value, value_basis, value_mean, value_square)
    low_output, output_first, output_second = moments(gradient_output, output_basis, output_mean, output_square)
    squares = jnp.sum(low_query * low_query) + jnp.sum(low_value * low_value) + jnp.sum(low_output * low_output)
    factor = 1.0 / jnp.sqrt(squares / (3.0 * MODEL * CELL) + floor_mean)
    query_step = -factor * low_query
    value_step = -factor * low_value
    output_step = -factor * low_output
    query_copy = (query_weight + learn_rate * query_step).astype(jnp.bfloat16)
    value_copy = (value_weight + learn_rate * value_step).astype(jnp.bfloat16)
    output_copy = (output_weight + learn_rate * output_step).astype(jnp.bfloat16)
    return (query_step, value_step, output_step, query_copy, value_copy, output_copy, query_first, value_first, output_first, query_second, value_second, output_second)
```

```python
import jax
import jax.numpy as jnp
from jax import lax
from jax.sharding import PartitionSpec as P

MODEL = 4096
CELL = 2048

beta_first = 0.8
beta_second = 0.9
floor_mean = 0.005
learn_rate = 0.05


def dot00(a, b):
    return lax.dot_general(a, b, (((0,), (0,)), ((), ())), preferred_element_type=jnp.float32)


def local(x, c, gq, gv, go, wq, wv, wo, bq, bv, bo, mq, mv, mo, sq, sv, so):
    bf = jnp.bfloat16
    f32 = jnp.float32
    bpack = jnp.concatenate(
        [jnp.concatenate([bq, bv], 1), jnp.concatenate([bo[:64], bo[64:]], 1)], 0
    )
    ball = lax.all_gather(bpack, "fs")
    wpack = jnp.concatenate(
        [jnp.concatenate([wq, wv], 1).astype(bf), wo.astype(bf)], 0
    )
    wall = lax.all_gather(wpack, "fs")
    bqv = ball[:, :256].reshape(4096, 256)
    bof = jnp.concatenate([ball[:, 256:, :128], ball[:, 256:, 128:]], 1).reshape(2048, 128)
    xb = jnp.dot(x, bqv, preferred_element_type=f32)
    cb = jnp.dot(c, bof, preferred_element_type=f32)

    def split(a):
        hi = a.astype(bf)
        return hi, (a - hi.astype(f32)).astype(bf)

    def proj(a, g):
        hi, lo = split(a)
        return dot00(hi, g) + dot00(lo, g)

    part = jnp.concatenate([proj(xb[:, :128], gq), proj(xb[:, 128:], gv), proj(cb, go)], 1)
    pieces = part.reshape(16, 8, 1024)
    mine = lax.all_to_all(pieces, "fs", 0, 0, tiled=True).sum(0)
    full = lax.all_gather(mine, "fs").reshape(128, 1024)
    mean = jnp.concatenate([mq, mv, mo], 1)
    square = jnp.concatenate([sq, sv, so], 1)
    first = beta_first * mean + (1.0 - beta_first) * full
    second = beta_second * square + (1.0 - beta_second) * full * full
    d = first / jnp.sqrt(second)
    H = lax.Precision.HIGHEST
    parts = 0.0
    for b, lo, hi in ((bqv[:, :128], 0, 256), (bqv[:, 128:], 256, 512), (bof, 512, 1024)):
        gram = dot00(b, b)
        dd = d[:, lo:hi]
        parts = parts + jnp.sum(dd * jnp.dot(gram, dd, precision=H))
    squares = lax.all_gather(parts, "tp").sum()
    factor = 1.0 / jnp.sqrt(squares / (3.0 * MODEL * CELL) + floor_mean)
    dn = -factor * d
    dq, dv, do = dn[:, :256], dn[:, 256:512], dn[:, 512:]

    def prod(b, dd):
        hi, lo = split(dd)
        return jnp.dot(b, hi, preferred_element_type=f32) + jnp.dot(b, lo, preferred_element_type=f32)

    steps = (prod(bq, dq), prod(bv, dv), prod(bo, do))

    def copy(w, b, dd):
        s = jnp.dot(b, dd.astype(bf), preferred_element_type=f32)
        return (w.astype(f32) + learn_rate * s).astype(bf)

    wqv = wall[:, :256]
    copies = (
        copy(wqv[:, :, :256].reshape(4096, 256), bqv[:, :128], dq),
        copy(wqv[:, :, 256:].reshape(4096, 256), bqv[:, 128:], dv),
        copy(wall[:, 256:].reshape(2048, 512), bof, do),
    )
    return (
        *steps,
        *copies,
        first[:, :256], first[:, 256:512], first[:, 512:],
        second[:, :256], second[:, 256:512], second[:, 512:],
    )


def solution(mesh):
    fs, both, tp = P("fs", None), P("fs", "tp"), P(None, "tp")
    in_specs = (fs, fs) + (both,) * 6 + (fs,) * 3 + (tp,) * 6
    out_specs = (both,) * 3 + (tp,) * 9
    return jax.shard_map(local, mesh=mesh, in_specs=in_specs, out_specs=out_specs, check_vma=False)
```

```python
import functools

import jax
import jax.numpy as jnp
from jax import lax
from jax.experimental import pallas as pl
from jax.experimental.pallas import tpu as pltpu
from jax.sharding import PartitionSpec as P

MODEL = 4096
CELL = 2048

beta_first = 0.8
beta_second = 0.9
floor_mean = 0.005
learn_rate = 0.05

f32 = jnp.float32
bf16 = jnp.bfloat16
HIGH = lax.Precision.HIGHEST
SIDE = 4
FS = SIDE * SIDE
TP = 8
B_ROWS = 320
W_ROWS = 384
B_CUTS = ((0, 48), (48, 32), (80, 48), (128, 32))
W_CUTS = ((0, 96), (96, 96), (192, 96), (288, 96))
OTHERS = [(dz, dx) for dz in range(SIDE) for dx in range(SIDE) if dz or dx]
MESH = pl.DeviceIdType.MESH


def slot(dz, dx):
    return (dz % SIDE) * SIDE + dx % SIDE


def link_plan(along_x, sign):
    near, far = ((0, 1), (2, 3)) if along_x else ((2, 3), (0, 1))
    which = 0 if sign > 0 else 1

    def at(far_off, near_off):
        return (far_off, near_off) if along_x else (near_off, far_off)

    steps = [(at(0, 0), near[0]), (at(0, 0), near[1]), (at(0, 0), far[0]), (at(0, 0), far[1])]
    steps.append((at(0, -sign), near[which]))
    steps += [(at(-1, 0), far[0]), (at(-1, 0), far[1]), (at(1, 0), far[0]), (at(1, 0), far[1])]
    steps.append((at(0, -sign), far[which]))
    steps += [(at(2, 0), far[0]), (at(2, 0), far[1])]
    steps += [(at(-1, -sign), far[which]), (at(1, -sign), far[which]), (at(2, -sign), far[which])]
    return steps


LINKS = [(True, 1), (True, -1), (False, 1), (False, -1)]
PLANS = [link_plan(*link) for link in LINKS]
STEPS = 15


def dot00(a, b):
    return lax.dot_general(a, b, (((0,), (0,)), ((), ())), preferred_element_type=f32)


def dot(a, b):
    return jnp.dot(a, b, preferred_element_type=f32)


class Torus:
    def __init__(self, buf, rows, send, recv, blk, neighbour):
        self.buf, self.rows, self.send, self.recv = buf, rows, send, recv
        self.blk, self.neighbour = blk, neighbour
        self.seen, self.started = set(), []

    def view(self, off, piece):
        start, size = self.rows[piece]
        return self.buf.at[self.blk(*off), pl.ds(start, size), :]

    def copy(self, off, piece, link, step, dest_off):
        ref = self.view(off, piece)
        return pltpu.make_async_remote_copy(
            src_ref=ref,
            dst_ref=ref,
            send_sem=self.send.at[link * STEPS + step],
            recv_sem=self.recv.at[slot(*dest_off) * 4 + piece],
            device_id={"fs": self.neighbour[link]},
            device_id_type=MESH,
        )

    def need(self, off, piece):
        off = (off[0] % SIDE, off[1] % SIDE)
        if off == (0, 0) or (off, piece) in self.seen:
            return
        self.seen.add((off, piece))
        ref = self.view(off, piece)
        pltpu.make_async_remote_copy(
            src_ref=ref,
            dst_ref=ref,
            send_sem=self.send.at[0],
            recv_sem=self.recv.at[slot(*off) * 4 + piece],
            device_id={"fs": self.neighbour[0]},
            device_id_type=MESH,
        ).wait_recv()

    def step(self, s):
        for link, (along_x, sign) in enumerate(LINKS):
            off, piece = PLANS[link][s]
            self.need(off, piece)
            dest = (off[0], off[1] - sign) if along_x else (off[0] - sign, off[1])
            c = self.copy(off, piece, link, s, dest)
            c.start()
            self.started.append(c)

    def block(self, off):
        for piece in range(4):
            self.need(off, piece)

    def finish(self):
        for c in self.started:
            c.wait_send()


def gather_kernel(
    x_h, c_h, gq_h, gv_h, go_h, wq_h, wv_h, wo_h, bq_h, bv_h, bo_h,
    mq_h, mv_h, mo_h, sq_h, sv_h, so_h,
    wall, ball, dcopy, stq, stv, sto, f1q, f1v, f1o, f2q, f2v, f2o,
    x, c, gq, gv, go, wqv, wo, mean, square,
    xb, cb, hl, part, psend, precv, pall, gram, d, sqs,
    lsem, wsend, wrecv, bsend, brecv, psems, psemr, rsend, rrecv, asend, arecv, ssend, srecv,
):
    f = lax.axis_index("fs")
    t = lax.axis_index("tp")
    z, xx = f // SIDE, lax.rem(f, SIDE)
    core = lax.rem(t, 2)

    def blk(dz, dx):
        return lax.rem(z + (dz % SIDE), SIDE) * SIDE + lax.rem(xx + (dx % SIDE), SIDE)

    n = [0]

    def load(src, dst):
        cp = pltpu.make_async_copy(src, dst, lsem.at[n[0]])
        n[0] += 1
        cp.start()
        return cp

    base_in = [
        load(bq_h, ball.at[f, pl.ds(0, 256), pl.ds(0, 128)]),
        load(bv_h, ball.at[f, pl.ds(0, 256), pl.ds(128, 128)]),
        load(bo_h.at[pl.ds(0, 64), :], ball.at[f, pl.ds(256, 64), pl.ds(0, 128)]),
        load(bo_h.at[pl.ds(64, 64), :], ball.at[f, pl.ds(256, 64), pl.ds(128, 128)]),
    ]
    w_in = [
        load(wq_h, wqv.at[:, pl.ds(0, 256)]),
        load(wv_h, wqv.at[:, pl.ds(256, 256)]),
        load(wo_h, wo),
    ]
    x_in = [load(x_h, x), load(c_h, c)]
    g_in = [load(gq_h, gq), load(gv_h, gv), load(go_h, go)]
    m_in = [
        load(mq_h, mean.at[:, pl.ds(0, 256)]),
        load(mv_h, mean.at[:, pl.ds(256, 256)]),
        load(mo_h, mean.at[:, pl.ds(512, 512)]),
        load(sq_h, square.at[:, pl.ds(0, 256)]),
        load(sv_h, square.at[:, pl.ds(256, 256)]),
        load(so_h, square.at[:, pl.ds(512, 512)]),
    ]

    barrier = pltpu.get_barrier_semaphore()
    for off in OTHERS:
        pl.semaphore_signal(barrier, inc=1, device_id={"fs": blk(*off)}, device_id_type=MESH)
    for r in range(1, TP):
        pl.semaphore_signal(
            barrier, inc=1, device_id={"tp": lax.rem(t + r, TP)}, device_id_type=MESH
        )
    for cp in w_in:
        cp.wait()
    wall[f, 0:256, :] = wqv[...].astype(bf16)
    wall[f, 256:384, :] = wo[...].astype(bf16)
    for cp in base_in:
        cp.wait()
    pl.semaphore_wait(barrier, FS - 1 + TP - 1)

    neighbour = [blk(0, 1), blk(0, -1), blk(1, 0), blk(-1, 0)]
    half = pl.multiple_of(core * 160, 16)
    brows = [(pl.multiple_of(half + start, 16), size) for start, size in B_CUTS]
    bases = Torus(ball, brows, bsend, brecv, blk, neighbour)
    weights = Torus(wall, W_CUTS, wsend, wrecv, blk, neighbour)

    other = t + 1 - 2 * core
    passed = []

    def partner(off, start):
        rows = pl.ds(pl.multiple_of(start * 160, 16), 160)
        ref = ball.at[blk(*off), rows, :]
        return pltpu.make_async_remote_copy(
            src_ref=ref,
            dst_ref=ref,
            send_sem=psems.at[slot(*off)],
            recv_sem=psemr.at[slot(*off)],
            device_id={"tp": other},
            device_id_type=MESH,
        )

    def hand_over(offs):
        for off in offs:
            bases.block(off)
            cp = partner(off, core)
            cp.start()
            passed.append(cp)

    def project(offs, first=False):
        for off in offs:
            b = blk(*off)
            if off != (0, 0):
                partner(off, 1 - core).wait_recv()
            xc = pl.ds(pl.multiple_of(b * 256, 256), 256)
            cc = pl.ds(pl.multiple_of(b * 128, 128), 128)
            bo = jnp.concatenate([ball[b, 256:320, 0:128], ball[b, 256:320, 128:256]], axis=0)
            px = dot(x[:, xc], ball[b, 0:256, :])
            pc = dot(c[:, cc], bo)
            if first and off == offs[0]:
                xb[...] = px
                cb[...] = pc
            else:
                xb[...] += px
                cb[...] += pc

    near = [(0, 1), (0, -1), (1, 0), (-1, 0)]
    middle = [(-1, -1), (-1, 1), (1, -1), (1, 1), (0, 2), (2, 0)]
    last = [(-1, 2), (1, 2), (2, -1), (2, 1), (2, 2)]

    for s in range(4):
        bases.step(s)
    weights.step(0)
    for s in range(4, 10):
        bases.step(s)
    hand_over(near)
    for cp in x_in:
        cp.wait()
    project([(0, 0)], first=True)
    project(near)
    for s in range(10, 14):
        bases.step(s)
    hand_over(middle)
    bases.step(14)
    weights.step(1)
    weights.step(2)
    project(middle)
    hand_over(last)
    weights.step(3)
    project(last)

    for cp in g_in:
        cp.wait()

    def split(a, at):
        hi = a.astype(bf16)
        hl[:, at : at + 128] = hi
        hl[:, at + 128 : at + 256] = (a - hi.astype(f32)).astype(bf16)

    split(xb[:, 0:128], 0)
    split(xb[:, 128:256], 256)
    split(cb[...], 512)
    for at, g, lo, hi in ((0, gq, 0, 256), (256, gv, 256, 512), (512, go, 512, 1024)):
        both = dot00(hl[:, at : at + 256], g[...])
        part[:, lo:hi] = both[0:128] + both[128:256]
    for j in range(FS):
        r, cc = 16 * (j // 2), 512 * (j % 2)
        psend[j] = part[r : r + 16, cc : cc + 512].astype(bf16)

    gq_sum = jnp.zeros((256, 256), f32)
    go_sum = jnp.zeros((128, 128), f32)
    for j in range(FS):
        bqv = ball[j, 0:256, :]
        bo = jnp.concatenate([ball[j, 256:320, 0:128], ball[j, 256:320, 128:256]], axis=0)
        gq_sum += dot00(bqv, bqv)
        go_sum += dot00(bo, bo)
    gram[0] = gq_sum[0:128, 0:128]
    gram[1] = gq_sum[128:256, 128:256]
    gram[2] = go_sum

    def to_peer(src, dst, send, recv, off):
        return pltpu.make_async_remote_copy(
            src_ref=src,
            dst_ref=dst,
            send_sem=send.at[slot(*off)],
            recv_sem=recv.at[slot(-off[0], -off[1])],
            device_id={"fs": blk(*off)},
            device_id_type=MESH,
        )

    scattered = []
    for off in OTHERS:
        cp = to_peer(psend.at[blk(*off)], precv.at[f], rsend, rrecv, off)
        cp.start()
        scattered.append(cp)
    weights.step(4)
    precv[f] = psend[f]
    for off in OTHERS:
        b = blk(*off)
        to_peer(psend.at[b], precv.at[b], rsend, rrecv, (-off[0], -off[1])).wait_recv()
    total = precv[0].astype(f32)
    for j in range(1, FS):
        total += precv[j].astype(f32)
    pall[f] = total.astype(bf16)
    weights.step(5)
    gathered = []
    for off in OTHERS:
        cp = to_peer(pall.at[f], pall.at[f], asend, arecv, off)
        cp.start()
        gathered.append(cp)
    weights.step(6)
    weights.step(7)
    for cp in m_in:
        cp.wait()
    for off in OTHERS:
        b = blk(*off)
        to_peer(pall.at[b], pall.at[b], asend, arecv, (-off[0], -off[1])).wait_recv()

    for j in range(FS):
        r, cc = 16 * (j // 2), 512 * (j % 2)
        rows = slice(r, r + 16)
        p = pall[j].astype(f32)
        one = beta_first * mean[rows, cc : cc + 512] + (1.0 - beta_first) * p
        two = beta_second * square[rows, cc : cc + 512] + (1.0 - beta_second) * p * p
        if j % 2:
            f1o[rows, :] = one
            f2o[rows, :] = two
        else:
            f1q[rows, :] = one[:, 0:256]
            f1v[rows, :] = one[:, 256:512]
            f2q[rows, :] = two[:, 0:256]
            f2v[rows, :] = two[:, 256:512]
        d[rows, cc : cc + 512] = one / jnp.sqrt(two)

    sums = jnp.zeros((1, 1), f32)
    for i, (lo, hi) in enumerate(((0, 256), (256, 512), (512, 1024))):
        dd = d[:, lo:hi]
        gd = jnp.dot(gram[i], dd, precision=HIGH, preferred_element_type=f32)
        sums += jnp.sum(dd * gd, keepdims=True)
    sqs[t] = jnp.broadcast_to(sums, (8, 128))
    weights.step(8)
    weights.step(9)

    def to_tp(src, r):
        return pltpu.make_async_remote_copy(
            src_ref=src,
            dst_ref=src,
            send_sem=ssend.at[r],
            recv_sem=srecv.at[(-r) % TP],
            device_id={"tp": lax.rem(t + r, TP)},
            device_id_type=MESH,
        )

    summed = []
    for r in range(1, TP):
        cp = to_tp(sqs.at[t], r)
        cp.start()
        summed.append(cp)
    weights.step(10)
    for r in range(1, TP):
        to_tp(sqs.at[lax.rem(t + r, TP)], TP - r).wait_recv()
    squares = sqs[0]
    for i in range(1, TP):
        squares += sqs[i]
    factor = 1.0 / jnp.sqrt(squares[0:1, 0:1] / (3.0 * MODEL * CELL) + floor_mean)
    dn = -factor * d[...]
    dcopy[...] = (learn_rate * dn).astype(bf16)
    weights.step(11)
    hi = dn.astype(bf16)
    lo = (dn - hi.astype(f32)).astype(bf16)
    bq = ball[f, 0:256, 0:128]
    bv = ball[f, 0:256, 128:256]
    bo = jnp.concatenate([ball[f, 256:320, 0:128], ball[f, 256:320, 128:256]], axis=0)
    stq[...] = dot(bq, hi[:, 0:256]) + dot(bq, lo[:, 0:256])
    stv[...] = dot(bv, hi[:, 256:512]) + dot(bv, lo[:, 256:512])
    sto[...] = dot(bo, hi[:, 512:1024]) + dot(bo, lo[:, 512:1024])
    for s in range(12, 15):
        weights.step(s)
    for off in OTHERS:
        weights.block(off)
    bases.finish()
    weights.finish()
    for cp in passed + scattered + gathered + summed:
        cp.wait_send()


def finish_kernel(
    wall, ball, dcopy, stq, stv, sto, f1q, f1v, f1o, f2q, f2v, f2o,
    o_stq, o_stv, o_sto, o_q, o_v, o_o, o_f1q, o_f1v, o_f1o, o_f2q, o_f2v, o_f2o,
    cq, cv, co, sem, csem,
):
    plain = [
        pltpu.make_async_copy(src, dst, sem.at[i])
        for i, (src, dst) in enumerate(
            (
                (stq, o_stq), (stv, o_stv), (sto, o_sto), (f1q, o_f1q), (f1v, o_f1v),
                (f1o, o_f1o), (f2q, o_f2q), (f2v, o_f2v), (f2o, o_f2o),
            )
        )
    ]
    for cp in plain:
        cp.start()
    sent = []
    for k in range(FS):
        bo = jnp.concatenate([ball[k, 256:320, 0:128], ball[k, 256:320, 128:256]], axis=0)
        wq = wall[k, 0:256, 0:256].astype(f32)
        cq[k * 256 : k * 256 + 256, :] = (
            wq + dot(ball[k, 0:256, 0:128], dcopy[:, 0:256])
        ).astype(bf16)
        wv = wall[k, 0:256, 256:512].astype(f32)
        cv[k * 256 : k * 256 + 256, :] = (
            wv + dot(ball[k, 0:256, 128:256], dcopy[:, 256:512])
        ).astype(bf16)
        wo = wall[k, 256:384, :].astype(f32)
        co[k * 128 : k * 128 + 128, :] = (wo + dot(bo, dcopy[:, 512:1024])).astype(bf16)
        for i, (src, dst, n) in enumerate(((cq, o_q, 256), (cv, o_v, 256), (co, o_o, 128))):
            cp = pltpu.make_async_copy(
                src.at[pl.ds(k * n, n), :], dst.at[pl.ds(k * n, n), :], csem.at[k * 3 + i]
            )
            cp.start()
            sent.append(cp)
    for cp in plain + sent:
        cp.wait()


def local(*args):
    tokens = args[0].shape[0]
    any_spec = pl.BlockSpec(memory_space=pl.ANY)
    vmem_spec = pl.BlockSpec(memory_space=pltpu.VMEM)
    mids = [
        ((FS, W_ROWS, 512), bf16),
        ((FS, B_ROWS, 256), bf16),
        ((128, 1024), bf16),
        ((256, 256), f32),
        ((256, 256), f32),
        ((128, 512), f32),
        ((128, 256), f32),
        ((128, 256), f32),
        ((128, 512), f32),
        ((128, 256), f32),
        ((128, 256), f32),
        ((128, 512), f32),
    ]
    dma = pltpu.SemaphoreType.DMA
    mid = pl.pallas_call(
        gather_kernel,
        out_shape=[pltpu.VMEM(s, t) for s, t in mids],
        in_specs=[any_spec] * 17,
        out_specs=[vmem_spec] * len(mids),
        scratch_shapes=[
            pltpu.VMEM((tokens, MODEL), bf16),
            pltpu.VMEM((tokens, CELL), bf16),
            pltpu.VMEM((tokens, 256), bf16),
            pltpu.VMEM((tokens, 256), bf16),
            pltpu.VMEM((tokens, 512), bf16),
            pltpu.VMEM((256, 512), f32),
            pltpu.VMEM((128, 512), f32),
            pltpu.VMEM((128, 1024), f32),
            pltpu.VMEM((128, 1024), f32),
            pltpu.VMEM((tokens, 256), f32),
            pltpu.VMEM((tokens, 128), f32),
            pltpu.VMEM((tokens, 768), bf16),
            pltpu.VMEM((128, 1024), f32),
            pltpu.VMEM((FS, 16, 512), bf16),
            pltpu.VMEM((FS, 16, 512), bf16),
            pltpu.VMEM((FS, 16, 512), bf16),
            pltpu.VMEM((3, 128, 128), f32),
            pltpu.VMEM((128, 1024), f32),
            pltpu.VMEM((TP, 8, 128), f32),
            dma((18,)),
            dma((60,)), dma((64,)), dma((60,)), dma((64,)), dma((16,)), dma((16,)),
            dma((16,)), dma((16,)), dma((16,)), dma((16,)), dma((8,)), dma((8,)),
        ],
        compiler_params=pltpu.CompilerParams(
            collective_id=0, has_side_effects=True, vmem_limit_bytes=48 * 1024 * 1024
        ),
        name="gather_and_reduce",
    )(*args)
    outs = [
        ((256, 256), f32), ((256, 256), f32), ((128, 512), f32),
        ((MODEL, 256), bf16), ((MODEL, 256), bf16), ((CELL, 512), bf16),
        ((128, 256), f32), ((128, 256), f32), ((128, 512), f32),
        ((128, 256), f32), ((128, 256), f32), ((128, 512), f32),
    ]
    return tuple(
        pl.pallas_call(
            finish_kernel,
            out_shape=[jax.ShapeDtypeStruct(s, t) for s, t in outs],
            in_specs=[vmem_spec] * len(mids),
            out_specs=[any_spec] * len(outs),
            scratch_shapes=[
                pltpu.VMEM((MODEL, 256), bf16),
                pltpu.VMEM((MODEL, 256), bf16),
                pltpu.VMEM((CELL, 512), bf16),
                dma((9,)),
                dma((48,)),
            ],
            compiler_params=pltpu.CompilerParams(vmem_limit_bytes=40 * 1024 * 1024),
            name="write_copies",
        )(*mid)
    )


def solution(mesh):
    fs, both, tp = P("fs", None), P("fs", "tp"), P(None, "tp")
    in_specs = (fs, fs) + (both,) * 6 + (fs,) * 3 + (tp,) * 6
    out_specs = (both,) * 3 + (tp,) * 9
    return jax.shard_map(local, mesh=mesh, in_specs=in_specs, out_specs=out_specs, check_vma=False)
```

```python
import functools

import jax
import jax.numpy as jnp
from jax import lax
from jax.experimental import pallas as pl
from jax.experimental.pallas import tpu as pltpu
from jax.sharding import PartitionSpec as P

MODEL = 4096
CELL = 2048

beta_first = 0.8
beta_second = 0.9
floor_mean = 0.005
learn_rate = 0.05

f32 = jnp.float32
bf16 = jnp.bfloat16
HIGH = lax.Precision.HIGHEST
SIDE = 4
FS = SIDE * SIDE
TP = 8
B_ROWS = 320
W_ROWS = 384
SLICE = B_ROWS // TP
W_CUTS = ((0, 96), (96, 96), (192, 96), (288, 96))
NEAR = [(0, 1), (0, -1), (1, 0), (-1, 0)]
MIDDLE = [(-1, -1), (-1, 1), (1, -1), (1, 1), (0, 2), (2, 0)]
FAR = [(-1, 2), (1, 2), (2, -1), (2, 1), (2, 2)]
OTHERS = NEAR + MIDDLE + FAR
MESH = pl.DeviceIdType.MESH


def slot(dz, dx):
    return (dz % SIDE) * SIDE + dx % SIDE


def link_plan(along_x, sign):
    near, far = ((0, 1), (2, 3)) if along_x else ((2, 3), (0, 1))
    which = 0 if sign > 0 else 1

    def at(far_off, near_off):
        return (far_off, near_off) if along_x else (near_off, far_off)

    steps = [(at(0, 0), near[0]), (at(0, 0), near[1]), (at(0, 0), far[0]), (at(0, 0), far[1])]
    steps.append((at(0, -sign), near[which]))
    steps += [(at(-1, 0), far[0]), (at(-1, 0), far[1]), (at(1, 0), far[0]), (at(1, 0), far[1])]
    steps.append((at(0, -sign), far[which]))
    steps += [(at(2, 0), far[0]), (at(2, 0), far[1])]
    steps += [(at(-1, -sign), far[which]), (at(1, -sign), far[which]), (at(2, -sign), far[which])]
    return steps


LINKS = [(True, 1), (True, -1), (False, 1), (False, -1)]
PLANS = [link_plan(*link) for link in LINKS]
STEPS = 15


def dot00(a, b):
    return lax.dot_general(a, b, (((0,), (0,)), ((), ())), preferred_element_type=f32)


def dot(a, b):
    return jnp.dot(a, b, preferred_element_type=f32)


class Torus:
    def __init__(self, buf, rows, send, recv, blk, neighbour):
        self.buf, self.rows, self.send, self.recv = buf, rows, send, recv
        self.blk, self.neighbour = blk, neighbour
        self.seen, self.started = set(), []

    def view(self, off, piece):
        start, size = self.rows[piece]
        return self.buf.at[self.blk(*off), pl.ds(start, size), :]

    def copy(self, off, piece, link, step, dest_off):
        ref = self.view(off, piece)
        return pltpu.make_async_remote_copy(
            src_ref=ref,
            dst_ref=ref,
            send_sem=self.send.at[link * STEPS + step],
            recv_sem=self.recv.at[slot(*dest_off) * 4 + piece],
            device_id={"fs": self.neighbour[link]},
            device_id_type=MESH,
        )

    def need(self, off, piece):
        off = (off[0] % SIDE, off[1] % SIDE)
        if off == (0, 0) or (off, piece) in self.seen:
            return
        self.seen.add((off, piece))
        ref = self.view(off, piece)
        pltpu.make_async_remote_copy(
            src_ref=ref,
            dst_ref=ref,
            send_sem=self.send.at[0],
            recv_sem=self.recv.at[slot(*off) * 4 + piece],
            device_id={"fs": self.neighbour[0]},
            device_id_type=MESH,
        ).wait_recv()

    def step(self, s):
        for link, (along_x, sign) in enumerate(LINKS):
            off, piece = PLANS[link][s]
            self.need(off, piece)
            dest = (off[0], off[1] - sign) if along_x else (off[0] - sign, off[1])
            c = self.copy(off, piece, link, s, dest)
            c.start()
            self.started.append(c)

    def block(self, off):
        for piece in range(4):
            self.need(off, piece)

    def finish(self):
        for c in self.started:
            c.wait_send()


def gather_kernel(
    x_h, c_h, gq_h, gv_h, go_h, wq_h, wv_h, wo_h, bq_h, bv_h, bo_h,
    mq_h, mv_h, mo_h, sq_h, sv_h, so_h,
    wall, ball, dcopy, stq, stv, sto, f1q, f1v, f1o, f2q, f2v, f2o,
    x, c, gq, gv, go, wqv, wo, mean, square,
    xb, cb, hl, part, psend, precv, pall, gram, d, sqs,
    lsem, wsend, wrecv, bsend, brecv, psems, psemr, ysend, yrecv, rsend, rrecv, asend, arecv, ssend, srecv,
):
    f = lax.axis_index("fs")
    t = lax.axis_index("tp")
    z, xx = f // SIDE, lax.rem(f, SIDE)
    core = lax.rem(t, 2)

    def blk(dz, dx):
        return lax.rem(z + (dz % SIDE), SIDE) * SIDE + lax.rem(xx + (dx % SIDE), SIDE)

    n = [0]

    def load(src, dst):
        cp = pltpu.make_async_copy(src, dst, lsem.at[n[0]])
        n[0] += 1
        cp.start()
        return cp

    base_in = [
        load(bq_h, ball.at[f, pl.ds(0, 256), pl.ds(0, 128)]),
        load(bv_h, ball.at[f, pl.ds(0, 256), pl.ds(128, 128)]),
        load(bo_h.at[pl.ds(0, 64), :], ball.at[f, pl.ds(256, 64), pl.ds(0, 128)]),
        load(bo_h.at[pl.ds(64, 64), :], ball.at[f, pl.ds(256, 64), pl.ds(128, 128)]),
    ]
    w_in = [
        load(wq_h, wqv.at[:, pl.ds(0, 256)]),
        load(wv_h, wqv.at[:, pl.ds(256, 256)]),
        load(wo_h, wo),
    ]
    x_in = [load(x_h, x), load(c_h, c)]
    g_in = [load(gq_h, gq), load(gv_h, gv), load(go_h, go)]
    m_in = [
        load(mq_h, mean.at[:, pl.ds(0, 256)]),
        load(mv_h, mean.at[:, pl.ds(256, 256)]),
        load(mo_h, mean.at[:, pl.ds(512, 512)]),
        load(sq_h, square.at[:, pl.ds(0, 256)]),
        load(sv_h, square.at[:, pl.ds(256, 256)]),
        load(so_h, square.at[:, pl.ds(512, 512)]),
    ]

    barrier = pltpu.get_barrier_semaphore()
    for off in OTHERS:
        pl.semaphore_signal(barrier, inc=1, device_id={"fs": blk(*off)}, device_id_type=MESH)
    for r in range(1, TP):
        pl.semaphore_signal(
            barrier, inc=1, device_id={"tp": lax.rem(t + r, TP)}, device_id_type=MESH
        )
    for cp in w_in:
        cp.wait()
    wall[f, 0:256, :] = wqv[...].astype(bf16)
    wall[f, 256:384, :] = wo[...].astype(bf16)
    for cp in base_in:
        cp.wait()
    pl.semaphore_wait(barrier, FS - 1 + TP - 1)

    neighbour = [blk(0, 1), blk(0, -1), blk(1, 0), blk(-1, 0)]
    weights = Torus(wall, W_CUTS, wsend, wrecv, blk, neighbour)
    y = t // 2
    above, below = lax.rem(y + 1, SIDE), lax.rem(y + SIDE - 1, SIDE)
    copies = []

    def slice_rows(level, start, size):
        return pl.ds(pl.multiple_of((core * SIDE + level) * SLICE + start, 8), size)

    def spread(off, send_at, recv_at, rows, device_id, send, recv):
        ref = ball.at[blk(*off), rows, :]
        return pltpu.make_async_remote_copy(
            src_ref=ref,
            dst_ref=ref,
            send_sem=send.at[send_at],
            recv_sem=recv.at[recv_at],
            device_id=device_id,
            device_id_type=MESH,
        )

    def start(cp):
        cp.start()
        copies.append(cp)

    def in_plane(off, src, arriving):
        return spread(
            src, slot(*off), slot(*arriving), slice_rows(y, 0, SLICE), {"fs": blk(*off)}, bsend, brecv
        )

    def level(kind, off, y_of, cut, up):
        i = kind * FS + slot(*off)
        tp_at = (above if up else below) * 2 + core
        return spread(off, i, i, slice_rows(y_of, *cut), {"tp": tp_at}, ysend, yrecv)

    def cuts(off):
        half = 24 if OTHERS.index(off) % 2 else 16
        return (0, half), (half, SLICE - half)

    def send_levels(offs):
        for off in offs:
            in_plane(off, off, off).wait_recv()
            start(level(0, off, y, (0, SLICE), True))
            start(level(1, off, y, (0, SLICE), False))

    def relay_levels(offs):
        for off in offs:
            low, high = cuts(off)
            level(0, off, below, (0, SLICE), True).wait_recv()
            start(level(2, off, below, low, True))
            level(1, off, above, (0, SLICE), False).wait_recv()
            start(level(3, off, above, high, False))

    def partner(off, of_core):
        rows = pl.ds(pl.multiple_of(of_core * SIDE * SLICE, 8), SIDE * SLICE)
        i = slot(*off)
        return spread(off, i, i, rows, {"tp": t + 1 - 2 * core}, psems, psemr)

    def hand_over(offs):
        opposite = lax.rem(y + 2, SIDE)
        for off in offs:
            low, high = cuts(off)
            level(2, off, opposite, low, True).wait_recv()
            level(3, off, opposite, high, False).wait_recv()
            start(partner(off, core))

    def outputs_of(b):
        return jnp.concatenate([ball[b, 256:320, 0:128], ball[b, 256:320, 128:256]], axis=0)

    def project(offs, first=False):
        bs = [blk(*off) for off in offs]
        for off in offs:
            if off != (0, 0):
                partner(off, 1 - core).wait_recv()
        xs = [x[:, pl.ds(pl.multiple_of(b * 256, 256), 256)] for b in bs]
        cs = [c[:, pl.ds(pl.multiple_of(b * 128, 128), 128)] for b in bs]
        px = dot(
            jnp.concatenate(xs, axis=1), jnp.concatenate([ball[b, 0:256, :] for b in bs], axis=0)
        )
        pc = dot(jnp.concatenate(cs, axis=1), jnp.concatenate([outputs_of(b) for b in bs], axis=0))
        if first:
            xb[...] = px
            cb[...] = pc
        else:
            xb[...] += px
            cb[...] += pc

    for off in OTHERS:
        start(in_plane(off, (0, 0), (-off[0], -off[1])))
    for s in range(4):
        weights.step(s)
    for cp in x_in:
        cp.wait()
    project([(0, 0)], first=True)
    send_levels(NEAR)
    send_levels(MIDDLE)
    relay_levels(NEAR)
    send_levels(FAR)
    relay_levels(MIDDLE)
    weights.step(4)
    hand_over(NEAR)
    relay_levels(FAR)
    hand_over(MIDDLE)
    weights.step(5)
    project(NEAR[0:2])
    project(NEAR[2:4])
    hand_over(FAR)
    weights.step(6)
    project(MIDDLE[0:2])
    project(MIDDLE[2:4])
    project(MIDDLE[4:6])
    weights.step(7)
    project(FAR[0:2])
    project(FAR[2:4])
    project(FAR[4:5])

    for cp in g_in:
        cp.wait()

    def split(a, at):
        hi = a.astype(bf16)
        hl[:, at : at + 128] = hi
        hl[:, at + 128 : at + 256] = (a - hi.astype(f32)).astype(bf16)

    split(xb[:, 0:128], 0)
    split(xb[:, 128:256], 256)
    split(cb[...], 512)
    for at, g, lo, hi in ((0, gq, 0, 256), (256, gv, 256, 512), (512, go, 512, 1024)):
        both = dot00(hl[:, at : at + 256], g[...])
        part[:, lo:hi] = both[0:128] + both[128:256]
    for j in range(FS):
        r, cc = 16 * (j // 2), 512 * (j % 2)
        psend[j] = part[r : r + 16, cc : cc + 512].astype(bf16)

    def grams(js, first=False):
        gq_sum = jnp.zeros((256, 256), f32)
        go_sum = jnp.zeros((128, 128), f32)
        for j in js:
            bqv = ball[j, 0:256, :]
            bo = outputs_of(j)
            gq_sum += dot00(bqv, bqv)
            go_sum += dot00(bo, bo)
        for i, g in enumerate((gq_sum[0:128, 0:128], gq_sum[128:256, 128:256], go_sum)):
            gram[i] = g if first else gram[i] + g

    grams(range(0, 4), first=True)

    def to_peer(src, dst, send, recv, off):
        return pltpu.make_async_remote_copy(
            src_ref=src,
            dst_ref=dst,
            send_sem=send.at[slot(*off)],
            recv_sem=recv.at[slot(-off[0], -off[1])],
            device_id={"fs": blk(*off)},
            device_id_type=MESH,
        )

    scattered = []
    for off in OTHERS:
        cp = to_peer(psend.at[blk(*off)], precv.at[f], rsend, rrecv, off)
        cp.start()
        scattered.append(cp)
    weights.step(8)
    grams(range(4, FS))
    precv[f] = psend[f]
    for off in OTHERS:
        b = blk(*off)
        to_peer(psend.at[b], precv.at[b], rsend, rrecv, (-off[0], -off[1])).wait_recv()
    total = precv[0].astype(f32)
    for j in range(1, FS):
        total += precv[j].astype(f32)
    pall[f] = total.astype(bf16)
    gathered = []
    for off in OTHERS:
        cp = to_peer(pall.at[f], pall.at[f], asend, arecv, off)
        cp.start()
        gathered.append(cp)
    for s in range(9, 13):
        weights.step(s)
    for cp in m_in:
        cp.wait()
    for off in OTHERS:
        b = blk(*off)
        to_peer(pall.at[b], pall.at[b], asend, arecv, (-off[0], -off[1])).wait_recv()

    for j in range(FS):
        r, cc = 16 * (j // 2), 512 * (j % 2)
        rows = slice(r, r + 16)
        p = pall[j].astype(f32)
        one = beta_first * mean[rows, cc : cc + 512] + (1.0 - beta_first) * p
        two = beta_second * square[rows, cc : cc + 512] + (1.0 - beta_second) * p * p
        if j % 2:
            f1o[rows, :] = one
            f2o[rows, :] = two
        else:
            f1q[rows, :] = one[:, 0:256]
            f1v[rows, :] = one[:, 256:512]
            f2q[rows, :] = two[:, 0:256]
            f2v[rows, :] = two[:, 256:512]
        d[rows, cc : cc + 512] = one / jnp.sqrt(two)

    sums = jnp.zeros((1, 1), f32)
    for i, (lo, hi) in enumerate(((0, 256), (256, 512), (512, 1024))):
        dd = d[:, lo:hi]
        gd = jnp.dot(gram[i], dd, precision=HIGH, preferred_element_type=f32)
        sums += jnp.sum(dd * gd, keepdims=True)
    sqs[t] = jnp.broadcast_to(sums, (8, 128))

    def to_tp(src, r):
        return pltpu.make_async_remote_copy(
            src_ref=src,
            dst_ref=src,
            send_sem=ssend.at[r],
            recv_sem=srecv.at[(-r) % TP],
            device_id={"tp": lax.rem(t + r, TP)},
            device_id_type=MESH,
        )

    summed = []
    for r in range(1, TP):
        cp = to_tp(sqs.at[t], r)
        cp.start()
        summed.append(cp)
    weights.step(13)
    weights.step(14)
    for r in range(1, TP):
        to_tp(sqs.at[lax.rem(t + r, TP)], TP - r).wait_recv()
    squares = sqs[0]
    for i in range(1, TP):
        squares += sqs[i]
    factor = 1.0 / jnp.sqrt(squares[0:1, 0:1] / (3.0 * MODEL * CELL) + floor_mean)
    dn = -factor * d[...]
    dcopy[...] = (learn_rate * dn).astype(bf16)
    hi = dn.astype(bf16)
    lo = (dn - hi.astype(f32)).astype(bf16)
    bq = ball[f, 0:256, 0:128]
    bv = ball[f, 0:256, 128:256]
    bo = jnp.concatenate([ball[f, 256:320, 0:128], ball[f, 256:320, 128:256]], axis=0)
    stq[...] = dot(bq, hi[:, 0:256]) + dot(bq, lo[:, 0:256])
    stv[...] = dot(bv, hi[:, 256:512]) + dot(bv, lo[:, 256:512])
    sto[...] = dot(bo, hi[:, 512:1024]) + dot(bo, lo[:, 512:1024])
    for off in OTHERS:
        weights.block(off)
    weights.finish()
    for cp in copies + scattered + gathered + summed:
        cp.wait_send()


def finish_kernel(
    wall, ball, dcopy, stq, stv, sto, f1q, f1v, f1o, f2q, f2v, f2o,
    o_stq, o_stv, o_sto, o_q, o_v, o_o, o_f1q, o_f1v, o_f1o, o_f2q, o_f2v, o_f2o,
    cq, cv, co, sem, csem,
):
    plain = [
        pltpu.make_async_copy(src, dst, sem.at[i])
        for i, (src, dst) in enumerate(
            (
                (stq, o_stq), (stv, o_stv), (sto, o_sto), (f1q, o_f1q), (f1v, o_f1v),
                (f1o, o_f1o), (f2q, o_f2q), (f2v, o_f2v), (f2o, o_f2o),
            )
        )
    ]
    for cp in plain:
        cp.start()
    sent = []
    for k in range(FS):
        bo = jnp.concatenate([ball[k, 256:320, 0:128], ball[k, 256:320, 128:256]], axis=0)
        wq = wall[k, 0:256, 0:256].astype(f32)
        cq[k * 256 : k * 256 + 256, :] = (
            wq + dot(ball[k, 0:256, 0:128], dcopy[:, 0:256])
        ).astype(bf16)
        wv = wall[k, 0:256, 256:512].astype(f32)
        cv[k * 256 : k * 256 + 256, :] = (
            wv + dot(ball[k, 0:256, 128:256], dcopy[:, 256:512])
        ).astype(bf16)
        wo = wall[k, 256:384, :].astype(f32)
        co[k * 128 : k * 128 + 128, :] = (wo + dot(bo, dcopy[:, 512:1024])).astype(bf16)
        for i, (src, dst, n) in enumerate(((cq, o_q, 256), (cv, o_v, 256), (co, o_o, 128))):
            cp = pltpu.make_async_copy(
                src.at[pl.ds(k * n, n), :], dst.at[pl.ds(k * n, n), :], csem.at[k * 3 + i]
            )
            cp.start()
            sent.append(cp)
    for cp in plain + sent:
        cp.wait()


def local(*args):
    tokens = args[0].shape[0]
    any_spec = pl.BlockSpec(memory_space=pl.ANY)
    vmem_spec = pl.BlockSpec(memory_space=pltpu.VMEM)
    mids = [
        ((FS, W_ROWS, 512), bf16),
        ((FS, B_ROWS, 256), bf16),
        ((128, 1024), bf16),
        ((256, 256), f32),
        ((256, 256), f32),
        ((128, 512), f32),
        ((128, 256), f32),
        ((128, 256), f32),
        ((128, 512), f32),
        ((128, 256), f32),
        ((128, 256), f32),
        ((128, 512), f32),
    ]
    dma = pltpu.SemaphoreType.DMA
    mid = pl.pallas_call(
        gather_kernel,
        out_shape=[pltpu.VMEM(s, t) for s, t in mids],
        in_specs=[any_spec] * 17,
        out_specs=[vmem_spec] * len(mids),
        scratch_shapes=[
            pltpu.VMEM((tokens, MODEL), bf16),
            pltpu.VMEM((tokens, CELL), bf16),
            pltpu.VMEM((tokens, 256), bf16),
            pltpu.VMEM((tokens, 256), bf16),
            pltpu.VMEM((tokens, 512), bf16),
            pltpu.VMEM((256, 512), f32),
            pltpu.VMEM((128, 512), f32),
            pltpu.VMEM((128, 1024), f32),
            pltpu.VMEM((128, 1024), f32),
            pltpu.VMEM((tokens, 256), f32),
            pltpu.VMEM((tokens, 128), f32),
            pltpu.VMEM((tokens, 768), bf16),
            pltpu.VMEM((128, 1024), f32),
            pltpu.VMEM((FS, 16, 512), bf16),
            pltpu.VMEM((FS, 16, 512), bf16),
            pltpu.VMEM((FS, 16, 512), bf16),
            pltpu.VMEM((3, 128, 128), f32),
            pltpu.VMEM((128, 1024), f32),
            pltpu.VMEM((TP, 8, 128), f32),
            dma((18,)),
            dma((60,)), dma((64,)), dma((16,)), dma((16,)), dma((16,)), dma((16,)), dma((64,)), dma((64,)),
            dma((16,)), dma((16,)), dma((16,)), dma((16,)), dma((8,)), dma((8,)),
        ],
        compiler_params=pltpu.CompilerParams(
            collective_id=0, has_side_effects=True, vmem_limit_bytes=48 * 1024 * 1024
        ),
        name="gather_and_reduce",
    )(*args)
    outs = [
        ((256, 256), f32), ((256, 256), f32), ((128, 512), f32),
        ((MODEL, 256), bf16), ((MODEL, 256), bf16), ((CELL, 512), bf16),
        ((128, 256), f32), ((128, 256), f32), ((128, 512), f32),
        ((128, 256), f32), ((128, 256), f32), ((128, 512), f32),
    ]
    return tuple(
        pl.pallas_call(
            finish_kernel,
            out_shape=[jax.ShapeDtypeStruct(s, t) for s, t in outs],
            in_specs=[vmem_spec] * len(mids),
            out_specs=[any_spec] * len(outs),
            scratch_shapes=[
                pltpu.VMEM((MODEL, 256), bf16),
                pltpu.VMEM((MODEL, 256), bf16),
                pltpu.VMEM((CELL, 512), bf16),
                dma((9,)),
                dma((48,)),
            ],
            compiler_params=pltpu.CompilerParams(vmem_limit_bytes=12 * 1024 * 1024),
            name="write_copies",
        )(*mid)
    )


def solution(mesh):
    fs, both, tp = P("fs", None), P("fs", "tp"), P(None, "tp")
    in_specs = (fs, fs) + (both,) * 6 + (fs,) * 3 + (tp,) * 6
    out_specs = (both,) * 3 + (tp,) * 9
    return jax.shard_map(local, mesh=mesh, in_specs=in_specs, out_specs=out_specs, check_vma=False)
```

```python
import functools

import jax
import jax.numpy as jnp
from jax import lax
from jax.experimental import pallas as pl
from jax.experimental.pallas import tpu as pltpu
from jax.sharding import PartitionSpec as P

MODEL = 4096
CELL = 2048

beta_first = 0.8
beta_second = 0.9
floor_mean = 0.005
learn_rate = 0.05

f32 = jnp.float32
bf16 = jnp.bfloat16
HIGH = lax.Precision.HIGHEST
SIDE = 4
FS = SIDE * SIDE
TP = 8
B_ROWS = 320
W_ROWS = 384
COLS = 64
SLICE = B_ROWS // TP
W_CUTS = ((0, 96), (96, 96), (192, 96), (288, 96))
NEAR = [(0, 1), (0, -1), (1, 0), (-1, 0)]
ACROSS = [(0, 2), (2, 0)]
DIAGONAL = [(-1, -1), (-1, 1), (1, -1), (1, 1)]
FAR = [(-1, 2), (2, -1), (1, 2), (2, 1), (2, 2)]
GROUPS = (NEAR, ACROSS, DIAGONAL, FAR)
OTHERS = NEAR + ACROSS + DIAGONAL + FAR
MESH = pl.DeviceIdType.MESH


def slot(dz, dx):
    return (dz % SIDE) * SIDE + dx % SIDE


def link_plan(along_x, sign):
    near, far = ((0, 1), (2, 3)) if along_x else ((2, 3), (0, 1))
    which = 0 if sign > 0 else 1

    def at(far_off, near_off):
        return (far_off, near_off) if along_x else (near_off, far_off)

    steps = [(at(0, 0), near[0]), (at(0, 0), near[1]), (at(0, 0), far[0]), (at(0, 0), far[1])]
    steps.append((at(0, -sign), near[which]))
    steps += [(at(-1, 0), far[0]), (at(-1, 0), far[1]), (at(1, 0), far[0]), (at(1, 0), far[1])]
    steps.append((at(0, -sign), far[which]))
    steps += [(at(2, 0), far[0]), (at(2, 0), far[1])]
    steps += [(at(-1, -sign), far[which]), (at(1, -sign), far[which]), (at(2, -sign), far[which])]
    return steps


LINKS = [(True, 1), (True, -1), (False, 1), (False, -1)]
PLANS = [link_plan(*link) for link in LINKS]
STEPS = 15


def dot00(a, b):
    return lax.dot_general(a, b, (((0,), (0,)), ((), ())), preferred_element_type=f32)


def dot(a, b):
    return jnp.dot(a, b, preferred_element_type=f32)


def arrivals():
    got = {}
    for (along_x, sign), plan in zip(LINKS, PLANS):
        for s, (off, piece) in enumerate(plan):
            dest = (off[0], off[1] - sign) if along_x else (off[0] - sign, off[1])
            got[slot(*dest), piece] = s
    return got


ARRIVALS = arrivals()


class Torus:
    def __init__(self, buf, rows, send, recv, blk, neighbour):
        self.buf, self.rows, self.send, self.recv = buf, rows, send, recv
        self.blk, self.neighbour = blk, neighbour
        self.seen = set()

    def copy(self, src, dst, send, recv, link):
        return pltpu.make_async_remote_copy(
            src_ref=src,
            dst_ref=dst,
            send_sem=send,
            recv_sem=recv,
            device_id={"fs": self.neighbour[link]},
            device_id_type=MESH,
        )

    def need(self, off, piece):
        s = ARRIVALS.get((slot(*off), piece))
        if s is None or s in self.seen:
            return
        self.seen.add(s)
        block = self.buf.at[0]
        self.copy(block, block, self.send, self.recv.at[s], 0).wait_recv()

    def step(self, s):
        for link in range(len(LINKS)):
            off, piece = PLANS[link][s]
            self.need(off, piece)
            start, size = self.rows[piece]
            ref = self.buf.at[self.blk(*off), pl.ds(start, size), :]
            self.copy(ref, ref, self.send, self.recv.at[s], link).start()

    def block(self, off):
        for piece in range(4):
            self.need(off, piece)

    def finish(self):
        sent = self.buf.at[pl.ds(0, STEPS)]
        self.copy(sent, sent, self.send, self.recv.at[0], 0).wait_send()


def gather_kernel(
    x_h, c_h, gq_h, gv_h, go_h, wq_h, wv_h, wo_h, bq_h, bv_h, bo_h,
    mq_h, mv_h, mo_h, sq_h, sv_h, so_h,
    wall, ball, dcopy, stq, stv, sto, f1q, f1v, f1o, f2q, f2v, f2o,
    x, c, gq, gv, go, wqv, wo, mean, square,
    xb, cb, gt, hl, psend, precv, pall, gram, turned, d, sqf, sqs,
    lsem, wsend, wrecv, bsend, brecv, psems, psemr, ysend, yrecv, rsend, rrecv, asend, arecv,
    fsend, frecv, ssend, srecv,
):
    f = lax.axis_index("fs")
    t = lax.axis_index("tp")
    z, xx = f // SIDE, lax.rem(f, SIDE)
    core = lax.rem(t, 2)

    def blk(dz, dx):
        return lax.rem(z + (dz % SIDE), SIDE) * SIDE + lax.rem(xx + (dx % SIDE), SIDE)

    def load(src, dst, sem):
        pltpu.make_async_copy(src, dst, lsem.at[sem]).start()

    def loaded(ref, sem):
        pltpu.make_async_copy(ref, ref, lsem.at[sem]).wait()

    load(bq_h, ball.at[f, pl.ds(0, 256), pl.ds(0, 128)], 0)
    load(bv_h, ball.at[f, pl.ds(0, 256), pl.ds(128, 128)], 0)
    load(bo_h.at[pl.ds(0, 64), :], ball.at[f, pl.ds(256, 64), pl.ds(0, 128)], 0)
    load(bo_h.at[pl.ds(64, 64), :], ball.at[f, pl.ds(256, 64), pl.ds(128, 128)], 0)
    load(wq_h, wqv.at[:, pl.ds(0, 256)], 1)
    load(wv_h, wqv.at[:, pl.ds(256, 256)], 1)
    load(wo_h, wo, 2)
    load(x_h, x, 3)
    load(c_h, c, 4)
    load(gq_h, gq, 5)
    load(gv_h, gv, 6)
    load(go_h, go, 7)
    for at, mean_in, square_in in ((0, mq_h, sq_h), (256, mv_h, sv_h), (512, mo_h, so_h)):
        cols = pl.ds(at, mean_in.shape[1])
        load(mean_in, mean.at[:, cols], 8)
        load(square_in, square.at[:, cols], 9)

    barrier = pltpu.get_barrier_semaphore()
    for off in OTHERS:
        pl.semaphore_signal(barrier, inc=1, device_id={"fs": blk(*off)}, device_id_type=MESH)
    for r in range(1, TP):
        pl.semaphore_signal(
            barrier, inc=1, device_id={"tp": lax.rem(t + r, TP)}, device_id_type=MESH
        )
    loaded(ball.at[f], 0)
    pl.semaphore_wait(barrier, FS - 1 + TP - 1)

    neighbour = [blk(0, 1), blk(0, -1), blk(1, 0), blk(-1, 0)]
    weights = Torus(wall, W_CUTS, wsend, wrecv, blk, neighbour)
    y = t // 2
    above, below = lax.rem(y + 1, SIDE), lax.rem(y + SIDE - 1, SIDE)
    groups = GROUPS

    def slice_rows(level, start, size):
        return pl.ds(pl.multiple_of((core * SIDE + level) * SLICE + start, 8), size)

    def remote(src, dst, send, recv, device_id):
        return pltpu.make_async_remote_copy(
            src_ref=src,
            dst_ref=dst,
            send_sem=send,
            recv_sem=recv,
            device_id=device_id,
            device_id_type=MESH,
        )

    def received(ref, recv):
        remote(ref, ref, recv, recv, {"fs": neighbour[0]}).wait_recv()

    def sent(ref, send):
        remote(ref, ref, send, send, {"fs": neighbour[0]}).wait_send()

    def group_of(off):
        return [slot(*off) in [slot(*o) for o in g] for g in groups].index(True)

    def in_plane(off, start, size, to):
        arriving = (off[0] - to[0], off[1] - to[1])
        ref = ball.at[blk(*off), slice_rows(y, start, size), :]
        remote(ref, ref, bsend, brecv.at[group_of(arriving)], {"fs": blk(*to)}).start()

    def x_first(off):
        return 24 if (off[0] + off[1]) % 2 else 16

    def turn(blocks):
        for dz, dx in blocks:
            peers = [(1, 0), (-1, 0), (2, 0)] if dz == 0 else [(0, 1), (0, -1), (0, 2)]
            for to in peers:
                h = x_first((dz - to[0], dx - to[1]))
                in_plane((dz, dx), *((0, h) if dz == 0 else (h, SLICE - h)), to)

    def level(off, rows, up, recv):
        ref = ball.at[blk(*off), slice_rows(*rows), :]
        remote(ref, ref, ysend, recv, {"tp": (above if up else below) * 2 + core}).start()

    def send_levels(i):
        received(ball.at[pl.ds(0, len(groups[i])), pl.ds(0, SLICE), :], brecv.at[i])
        for off in groups[i]:
            level(off, (y, 0, SLICE), True, yrecv.at[i])
            level(off, (y, 0, SLICE), False, yrecv.at[i])

    def relay_levels(i):
        received(ball.at[pl.ds(0, len(groups[i])), pl.ds(0, 2 * SLICE), :], yrecv.at[i])
        for off in groups[i]:
            half = 24 if OTHERS.index(off) % 2 else 16
            level(off, (below, 0, half), True, yrecv.at[len(GROUPS) + i])
            level(off, (above, half, SLICE - half), False, yrecv.at[len(GROUPS) + i])

    def hand_over(i):
        received(ball.at[pl.ds(0, len(groups[i])), pl.ds(0, SLICE), :], yrecv.at[len(GROUPS) + i])
        rows = pl.ds(pl.multiple_of(core * SIDE * SLICE, 8), SIDE * SLICE)
        for off in groups[i]:
            ref = ball.at[blk(*off), rows, :]
            remote(ref, ref, psems, psemr.at[i], {"tp": t + 1 - 2 * core}).start()

    def handed(i):
        received(ball.at[pl.ds(0, len(groups[i])), pl.ds(0, SIDE * SLICE), :], psemr.at[i])

    def outputs_of(b):
        return jnp.concatenate([ball[b, 256:320, 0:128], ball[b, 256:320, 128:256]], axis=0)

    def project(offs, first=False):
        bs = [blk(*off) for off in offs]
        xs = [x[:, pl.ds(pl.multiple_of(b * 256, 256), 256)] for b in bs]
        cs = [c[:, pl.ds(pl.multiple_of(b * 128, 128), 128)] for b in bs]
        px = dot(
            jnp.concatenate(xs, axis=1), jnp.concatenate([ball[b, 0:256, :] for b in bs], axis=0)
        )
        pc = dot(jnp.concatenate(cs, axis=1), jnp.concatenate([outputs_of(b) for b in bs], axis=0))
        if first:
            xb[...] = px
            cb[...] = pc
        else:
            xb[...] += px
            cb[...] += pc

    for off in NEAR + ACROSS:
        in_plane((0, 0), 0, SLICE, off)
    loaded(wqv, 1)
    loaded(wo, 2)
    wall[f, 0:256, :] = wqv[...].astype(bf16)
    wall[f, 256:384, :] = wo[...].astype(bf16)
    weights.step(0)
    send_levels(0)
    turn(NEAR)
    send_levels(1)
    turn(ACROSS)
    for s in range(1, 4):
        weights.step(s)
    loaded(x, 3)
    loaded(c, 4)
    project([(0, 0)], first=True)
    relay_levels(0)
    send_levels(2)
    for g, sem, lo, hi in ((gq, 5, 0, 256), (gv, 6, 256, 512), (go, 7, 512, 1024)):
        loaded(g, sem)
        gt[lo:hi, :] = g[...].T
    relay_levels(1)
    send_levels(3)
    weights.step(4)
    hand_over(0)
    relay_levels(2)
    hand_over(1)
    weights.step(5)
    relay_levels(3)
    weights.step(6)
    handed(0)
    project(NEAR[0:2])
    project(NEAR[2:4])
    hand_over(2)
    weights.step(7)
    handed(1)
    project(ACROSS)
    hand_over(3)
    weights.step(8)
    handed(2)
    project(DIAGONAL[0:2])
    project(DIAGONAL[2:4])
    weights.step(9)
    handed(3)
    project(FAR[0:2])
    project(FAR[2:4])
    project(FAR[4:5])


    def split(a, at):
        hi = a.astype(bf16)
        hl[:, at : at + 128] = hi
        hl[:, at + 128 : at + 256] = (a - hi.astype(f32)).astype(bf16)

    split(xb[:, 0:128], 0)
    split(xb[:, 128:256], 256)
    split(cb[...], 512)
    for at, lo, hi in ((0, 0, 256), (256, 256, 512), (512, 512, 1024)):
        both = dot(gt[lo:hi, :], hl[:, at : at + 256])
        both = (both[:, 0:128] + both[:, 128:256]).astype(bf16)
        for j in range(lo // COLS, hi // COLS):
            psend[j] = both[j * COLS - lo : (j + 1) * COLS - lo, :]

    def grams(js, first=False):
        gq_sum = jnp.zeros((256, 256), f32)
        go_sum = jnp.zeros((128, 128), f32)
        for j in js:
            bqv = ball[j, 0:256, :]
            bo = outputs_of(j)
            gq_sum += dot00(bqv, bqv)
            go_sum += dot00(bo, bo)
        for i, g in enumerate((gq_sum[0:128, 0:128], gq_sum[128:256, 128:256], go_sum)):
            gram[i] = g if first else gram[i] + g

    grams(range(0, 1), first=True)

    def to_peer(src, dst, send, recv, off):
        remote(src, dst, send, recv, {"fs": blk(*off)}).start()

    for off in OTHERS:
        to_peer(psend.at[blk(*off)], precv.at[f], rsend, rrecv, off)
    weights.step(10)
    grams(range(1, FS))
    precv[f] = psend[f]
    loaded(mean, 8)
    loaded(square, 9)
    slab = pl.ds(pl.multiple_of((f // 2) * 128, 128), 128)
    turned[0] = mean[:, slab].T
    turned[1] = square[:, slab].T
    weights.step(11)
    peers = pl.ds(0, FS - 1)
    received(precv.at[peers], rrecv)
    total = precv[0].astype(f32)
    for j in range(1, FS):
        total += precv[j].astype(f32)
    total = total.astype(bf16)
    pall[f] = total

    def moments(p, mean_old, square_old):
        one = beta_first * mean_old + (1.0 - beta_first) * p
        two = beta_second * square_old + (1.0 - beta_second) * p * p
        return one, two, one / jnp.sqrt(two)

    own = pl.ds(pl.multiple_of(lax.rem(f, 2) * COLS, COLS), COLS)
    _, _, own_d = moments(total.astype(f32), turned[0, own, :], turned[1, own, :])
    gd = jnp.dot(
        own_d, gram[jnp.minimum(f // 4, 2)], precision=HIGH, preferred_element_type=f32
    )
    sqf[f] = jnp.broadcast_to(jnp.sum(own_d * gd, keepdims=True), (1, 128))
    for off in OTHERS:
        to_peer(sqf.at[f], sqf.at[f], fsend, frecv, off)
    for off in NEAR + ACROSS:
        to_peer(pall.at[f], pall.at[f], asend, arecv.at[0], off)
    weights.step(12)
    weights.step(13)
    received(sqf.at[peers], frecv)
    squares = sqf[0]
    for j in range(1, FS):
        squares += sqf[j]
    sqs[t] = squares

    for r in range(1, TP):
        remote(sqs.at[t], sqs.at[t], ssend, srecv, {"tp": lax.rem(t + r, TP)}).start()
    received(pall.at[pl.ds(0, len(NEAR + ACROSS))], arecv.at[0])
    upper, lower = pl.ds(0, COLS // 2), pl.ds(COLS // 2, COLS // 2)
    for step in (1, -1, 2):
        for to in (1, -1, 2):
            ref = pall.at[blk(0, step), upper, :]
            to_peer(ref, ref, asend, arecv.at[1], (to, 0))
            ref = pall.at[blk(step, 0), lower, :]
            to_peer(ref, ref, asend, arecv.at[1], (0, to))
    weights.step(14)
    received(pall.at[pl.ds(0, len(DIAGONAL + FAR))], arecv.at[1])
    firsts = [(f1q, 0), (f1q, 128), (f1v, 0), (f1v, 128)] + [(f1o, 128 * i) for i in range(4)]
    seconds = [(f2q, 0), (f2q, 128), (f2v, 0), (f2v, 128)] + [(f2o, 128 * i) for i in range(4)]
    for k in range(8):
        at = slice(128 * k, 128 * k + 128)
        p = jnp.concatenate([pall[2 * k], pall[2 * k + 1]], axis=0).astype(f32).T
        one, two, d[:, at] = moments(p, mean[:, at], square[:, at])
        ref, lo = firsts[k]
        ref[:, lo : lo + 128] = one
        ref, lo = seconds[k]
        ref[:, lo : lo + 128] = two
    hi = d[...].astype(bf16)
    lo = (d[...] - hi.astype(f32)).astype(bf16)
    bqv, bo = ball[f, 0:256, :], outputs_of(f)
    low_q = dot(bqv[:, 0:128], hi[:, 0:256]) + dot(bqv[:, 0:128], lo[:, 0:256])
    low_v = dot(bqv[:, 128:256], hi[:, 256:512]) + dot(bqv[:, 128:256], lo[:, 256:512])
    low_o = dot(bo, hi[:, 512:1024]) + dot(bo, lo[:, 512:1024])
    stq[...] = low_q
    stv[...] = low_v
    sto[...] = low_o
    received(sqs.at[pl.ds(0, TP - 1)], srecv)
    squares = sqs[0]
    for i in range(1, TP):
        squares += sqs[i]
    factor = 1.0 / jnp.sqrt(squares[0:1, 0:1] / (3.0 * MODEL * CELL) + floor_mean)
    dcopy[...] = (-learn_rate * factor * d[...]).astype(bf16)
    stq[...] = -factor * stq[...]
    stv[...] = -factor * stv[...]
    sto[...] = -factor * sto[...]
    for off in OTHERS:
        weights.block(off)
    weights.finish()
    blocks = pl.ds(0, FS - 1)
    sent(ball.at[pl.ds(0, len(NEAR + ACROSS)), pl.ds(0, SLICE), :], bsend)
    sent(ball.at[pl.ds(0, len(DIAGONAL + FAR)), pl.ds(0, SLICE), :], bsend)
    sent(ball.at[blocks, pl.ds(0, 3 * SLICE), :], ysend)
    sent(ball.at[blocks, pl.ds(0, SIDE * SLICE), :], psems)
    sent(psend.at[peers], rsend)
    sent(pall.at[peers], asend)
    sent(sqf.at[peers], fsend)
    sent(sqs.at[pl.ds(0, TP - 1)], ssend)


def finish_kernel(
    wall, ball, dcopy, stq, stv, sto, f1q, f1v, f1o, f2q, f2v, f2o,
    o_stq, o_stv, o_sto, o_q, o_v, o_o, o_f1q, o_f1v, o_f1o, o_f2q, o_f2v, o_f2o,
    cq, cv, co, sem, csem,
):
    plain = [
        pltpu.make_async_copy(src, dst, sem.at[i])
        for i, (src, dst) in enumerate(
            (
                (stq, o_stq), (stv, o_stv), (sto, o_sto), (f1q, o_f1q), (f1v, o_f1v),
                (f1o, o_f1o), (f2q, o_f2q), (f2v, o_f2v), (f2o, o_f2o),
            )
        )
    ]
    for cp in plain:
        cp.start()
    for k in range(FS):
        bo = jnp.concatenate([ball[k, 256:320, 0:128], ball[k, 256:320, 128:256]], axis=0)
        wq = wall[k, 0:256, 0:256].astype(f32)
        cq[k * 256 : k * 256 + 256, :] = (
            wq + dot(ball[k, 0:256, 0:128], dcopy[:, 0:256])
        ).astype(bf16)
        wv = wall[k, 0:256, 256:512].astype(f32)
        cv[k * 256 : k * 256 + 256, :] = (
            wv + dot(ball[k, 0:256, 128:256], dcopy[:, 256:512])
        ).astype(bf16)
        wo = wall[k, 256:384, :].astype(f32)
        co[k * 128 : k * 128 + 128, :] = (wo + dot(bo, dcopy[:, 512:1024])).astype(bf16)
        for i, (src, dst, n) in enumerate(((cq, o_q, 256), (cv, o_v, 256), (co, o_o, 128))):
            cp = pltpu.make_async_copy(
                src.at[pl.ds(k * n, n), :], dst.at[pl.ds(k * n, n), :], csem.at[i]
            )
            cp.start()
    for cp in plain:
        cp.wait()
    for i, (src, dst) in enumerate(((cq, o_q), (cv, o_v), (co, o_o))):
        pltpu.make_async_copy(src, dst, csem.at[i]).wait()


def local(*args):
    tokens = args[0].shape[0]
    any_spec = pl.BlockSpec(memory_space=pl.ANY)
    vmem_spec = pl.BlockSpec(memory_space=pltpu.VMEM)
    steps = [((256, 256), f32), ((256, 256), f32), ((128, 512), f32)]
    news = [((MODEL, 256), bf16), ((MODEL, 256), bf16), ((CELL, 512), bf16)]
    moment = [((128, 256), f32), ((128, 256), f32), ((128, 512), f32)]
    mids = [((FS, W_ROWS, 512), bf16), ((FS, B_ROWS, 256), bf16), ((128, 1024), bf16)]
    mids += steps + moment + moment
    outs = steps + news + moment + moment
    dma = pltpu.SemaphoreType.DMA
    mid = pl.pallas_call(
        gather_kernel,
        out_shape=[pltpu.VMEM(s, t) for s, t in mids],
        in_specs=[any_spec] * 17,
        out_specs=[vmem_spec] * len(mids),
        scratch_shapes=[
            pltpu.VMEM((tokens, MODEL), bf16),
            pltpu.VMEM((tokens, CELL), bf16),
            pltpu.VMEM((tokens, 256), bf16),
            pltpu.VMEM((tokens, 256), bf16),
            pltpu.VMEM((tokens, 512), bf16),
            pltpu.VMEM((256, 512), f32),
            pltpu.VMEM((128, 512), f32),
            pltpu.VMEM((128, 1024), f32),
            pltpu.VMEM((128, 1024), f32),
            pltpu.VMEM((tokens, 256), f32),
            pltpu.VMEM((tokens, 128), f32),
            pltpu.VMEM((1024, tokens), bf16),
            pltpu.VMEM((tokens, 768), bf16),
            pltpu.VMEM((FS, COLS, 128), bf16),
            pltpu.VMEM((FS, COLS, 128), bf16),
            pltpu.VMEM((FS, COLS, 128), bf16),
            pltpu.VMEM((3, 128, 128), f32),
            pltpu.VMEM((2, 128, 128), f32),
            pltpu.VMEM((128, 1024), f32),
            pltpu.VMEM((FS, 1, 128), f32),
            pltpu.VMEM((TP, 1, 128), f32),
            dma((10,)),
            dma, dma((STEPS,)), dma, dma((4,)), dma, dma((4,)), dma, dma((8,)),
            dma, dma, dma, dma((2,)), dma, dma, dma, dma,
        ],
        compiler_params=pltpu.CompilerParams(
            collective_id=0, has_side_effects=True, vmem_limit_bytes=50 * 1024 * 1024
        ),
        name="gather_and_reduce",
    )(*args)
    return tuple(
        pl.pallas_call(
            finish_kernel,
            out_shape=[jax.ShapeDtypeStruct(s, t) for s, t in outs],
            in_specs=[vmem_spec] * len(mids),
            out_specs=[any_spec] * len(outs),
            scratch_shapes=[
                pltpu.VMEM((MODEL, 256), bf16),
                pltpu.VMEM((MODEL, 256), bf16),
                pltpu.VMEM((CELL, 512), bf16),
                dma((9,)),
                dma((3,)),
            ],
            compiler_params=pltpu.CompilerParams(vmem_limit_bytes=12 * 1024 * 1024),
            name="write_copies",
        )(*mid)
    )


def solution(mesh):
    fs, both, tp = P("fs", None), P("fs", "tp"), P(None, "tp")
    in_specs = (fs, fs) + (both,) * 6 + (fs,) * 3 + (tp,) * 6
    out_specs = (both,) * 3 + (tp,) * 9
    return jax.shard_map(local, mesh=mesh, in_specs=in_specs, out_specs=out_specs, check_vma=False)
```

```python
import functools

import jax
import jax.numpy as jnp
from jax import lax
from jax.experimental import pallas as pl
from jax.experimental.pallas import tpu as pltpu
from jax.sharding import PartitionSpec as P

MODEL = 4096
CELL = 2048

beta_first = 0.8
beta_second = 0.9
floor_mean = 0.005
learn_rate = 0.05

f32 = jnp.float32
bf16 = jnp.bfloat16
HIGH = lax.Precision.HIGHEST
SIDE = 4
FS = SIDE * SIDE
TP = 8
B_ROWS = 320
W_ROWS = 384
COLS = 64
SLICES = (32, 48)
W_CUTS = ((0, 96), (96, 96), (192, 96), (288, 96))
NEAR = [(0, 1), (0, -1), (1, 0), (-1, 0)]
ACROSS = [(0, 2), (2, 0)]
DIAGONAL = [(-1, -1), (-1, 1), (1, -1), (1, 1)]
FAR = [(-1, 2), (2, -1), (1, 2), (2, 1), (2, 2)]
GROUPS = (NEAR, ACROSS, DIAGONAL, FAR)
OTHERS = NEAR + ACROSS + DIAGONAL + FAR
MESH = pl.DeviceIdType.MESH


def slot(dz, dx):
    return (dz % SIDE) * SIDE + dx % SIDE


def link_plan(along_x, sign):
    near, far = ((0, 1), (2, 3)) if along_x else ((2, 3), (0, 1))
    which = 0 if sign > 0 else 1

    def at(far_off, near_off):
        return (far_off, near_off) if along_x else (near_off, far_off)

    steps = [(at(0, 0), near[0]), (at(0, 0), near[1]), (at(0, 0), far[0]), (at(0, 0), far[1])]
    steps.append((at(0, -sign), near[which]))
    steps += [(at(-1, 0), far[0]), (at(-1, 0), far[1]), (at(1, 0), far[0]), (at(1, 0), far[1])]
    steps.append((at(0, -sign), far[which]))
    steps += [(at(2, 0), far[0]), (at(2, 0), far[1])]
    steps += [(at(-1, -sign), far[which]), (at(1, -sign), far[which]), (at(2, -sign), far[which])]
    return steps


LINKS = [(True, 1), (True, -1), (False, 1), (False, -1)]
PLANS = [link_plan(*link) for link in LINKS]
STEPS = 15


def dot00(a, b):
    return lax.dot_general(a, b, (((0,), (0,)), ((), ())), preferred_element_type=f32)


def dot(a, b):
    return jnp.dot(a, b, preferred_element_type=f32)


def arrivals():
    got = {}
    for (along_x, sign), plan in zip(LINKS, PLANS):
        for s, (off, piece) in enumerate(plan):
            dest = (off[0], off[1] - sign) if along_x else (off[0] - sign, off[1])
            got[slot(*dest), piece] = s
    return got


ARRIVALS = arrivals()


class Torus:
    def __init__(self, buf, rows, send, recv, blk, neighbour):
        self.buf, self.rows, self.send, self.recv = buf, rows, send, recv
        self.blk, self.neighbour = blk, neighbour
        self.seen = set()

    def copy(self, src, dst, send, recv, link):
        return pltpu.make_async_remote_copy(
            src_ref=src,
            dst_ref=dst,
            send_sem=send,
            recv_sem=recv,
            device_id={"fs": self.neighbour[link]},
            device_id_type=MESH,
        )

    def need(self, off, piece):
        s = ARRIVALS.get((slot(*off), piece))
        if s is None or s in self.seen:
            return
        self.seen.add(s)
        block = self.buf.at[0]
        self.copy(block, block, self.send, self.recv.at[s], 0).wait_recv()

    def step(self, s):
        for link in range(len(LINKS)):
            off, piece = PLANS[link][s]
            self.need(off, piece)
            start, size = self.rows[piece]
            ref = self.buf.at[self.blk(*off), pl.ds(start, size), :]
            self.copy(ref, ref, self.send, self.recv.at[s], link).start()

    def block(self, off):
        for piece in range(4):
            self.need(off, piece)

    def finish(self):
        sent = self.buf.at[pl.ds(0, STEPS)]
        self.copy(sent, sent, self.send, self.recv.at[0], 0).wait_send()


def gather_kernel(
    x_h, c_h, gq_h, gv_h, go_h, wq_h, wv_h, wo_h, bq_h, bv_h, bo_h,
    mq_h, mv_h, mo_h, sq_h, sv_h, so_h,
    wall, ball, dcopy, stq, stv, sto, f1q, f1v, f1o, f2q, f2v, f2o,
    x, c, gq, gv, go, wqv, wo, mean, square,
    xb, cb, gt, hl, psend, precv, pall, gram, turned, d, sqf, sqs,
    lsem, wsend, wrecv, bsend, brecv, psems, psemr, ysend, yrecv, rsend, rrecv, asend, arecv,
    fsend, frecv, ssend, srecv,
):
    f = lax.axis_index("fs")
    t = lax.axis_index("tp")
    z, xx = f // SIDE, lax.rem(f, SIDE)
    core = lax.rem(t, 2)

    def blk(dz, dx):
        return lax.rem(z + (dz % SIDE), SIDE) * SIDE + lax.rem(xx + (dx % SIDE), SIDE)

    def load(src, dst, sem):
        pltpu.make_async_copy(src, dst, lsem.at[sem]).start()

    def loaded(ref, sem):
        pltpu.make_async_copy(ref, ref, lsem.at[sem]).wait()

    load(bq_h, ball.at[f, pl.ds(0, 256), pl.ds(0, 128)], 0)
    load(bv_h, ball.at[f, pl.ds(0, 256), pl.ds(128, 128)], 0)
    load(bo_h.at[pl.ds(0, 64), :], ball.at[f, pl.ds(256, 64), pl.ds(0, 128)], 0)
    load(bo_h.at[pl.ds(64, 64), :], ball.at[f, pl.ds(256, 64), pl.ds(128, 128)], 0)
    load(wq_h, wqv.at[:, pl.ds(0, 256)], 1)
    load(wv_h, wqv.at[:, pl.ds(256, 256)], 1)
    load(wo_h, wo, 2)
    load(x_h, x, 3)
    load(c_h, c, 4)
    load(gq_h, gq, 5)
    load(gv_h, gv, 6)
    load(go_h, go, 7)
    for at, mean_in, square_in in ((0, mq_h, sq_h), (256, mv_h, sv_h), (512, mo_h, so_h)):
        cols = pl.ds(at, mean_in.shape[1])
        load(mean_in, mean.at[:, cols], 8)
        load(square_in, square.at[:, cols], 9)

    barrier = pltpu.get_barrier_semaphore()
    for off in OTHERS:
        pl.semaphore_signal(barrier, inc=1, device_id={"fs": blk(*off)}, device_id_type=MESH)
    for r in range(1, TP):
        pl.semaphore_signal(
            barrier, inc=1, device_id={"tp": lax.rem(t + r, TP)}, device_id_type=MESH
        )
    loaded(ball.at[f], 0)
    pl.semaphore_wait(barrier, FS - 1 + TP - 1)

    neighbour = [blk(0, 1), blk(0, -1), blk(1, 0), blk(-1, 0)]
    weights = Torus(wall, W_CUTS, wsend, wrecv, blk, neighbour)
    y = t // 2
    above, below = lax.rem(y + 1, SIDE), lax.rem(y + SIDE - 1, SIDE)
    groups = GROUPS

    def by_core(fn):
        for own in range(2):
            pl.when(core == own)(functools.partial(fn, own, SLICES[own]))

    def slice_rows(own, level, start, size):
        at = own * SIDE * SLICES[0] + level * SLICES[own] + start
        return pl.ds(pl.multiple_of(at, 8), size)

    def remote(src, dst, send, recv, device_id):
        return pltpu.make_async_remote_copy(
            src_ref=src,
            dst_ref=dst,
            send_sem=send,
            recv_sem=recv,
            device_id=device_id,
            device_id_type=MESH,
        )

    def received(ref, recv):
        remote(ref, ref, recv, recv, {"fs": neighbour[0]}).wait_recv()

    def sent(ref, send):
        remote(ref, ref, send, send, {"fs": neighbour[0]}).wait_send()

    def group_of(off):
        return [slot(*off) in [slot(*o) for o in g] for g in groups].index(True)

    def in_plane(own, off, start, size, to):
        arriving = (off[0] - to[0], off[1] - to[1])
        ref = ball.at[blk(*off), slice_rows(own, y, start, size), :]
        remote(ref, ref, bsend, brecv.at[group_of(arriving)], {"fs": blk(*to)}).start()

    def spread_own(own, size):
        for off in NEAR + ACROSS:
            in_plane(own, (0, 0), 0, size, off)

    def turn(blocks, own, size):
        for dz, dx in blocks:
            peers = [(1, 0), (-1, 0), (2, 0)] if dz == 0 else [(0, 1), (0, -1), (0, 2)]
            for to in peers:
                in_plane(own, (dz, dx), 0 if dz == 0 else size // 2, size // 2, to)

    def level(own, off, rows, up, recv):
        ref = ball.at[blk(*off), slice_rows(own, *rows), :]
        remote(ref, ref, ysend, recv, {"tp": (above if up else below) * 2 + core}).start()

    def send_levels(i, own, size):
        received(ball.at[pl.ds(0, len(groups[i])), pl.ds(0, size), :], brecv.at[i])
        for off in groups[i]:
            level(own, off, (y, 0, size), True, yrecv.at[i])
            level(own, off, (y, 0, size), False, yrecv.at[i])
        if i < 2:
            turn(groups[i], own, size)

    def relay_levels(i, own, size):
        received(ball.at[pl.ds(0, len(groups[i])), pl.ds(0, 2 * size), :], yrecv.at[i])
        for off in groups[i]:
            recv = yrecv.at[len(GROUPS) + i]
            level(own, off, (below, 0, size // 2), True, recv)
            level(own, off, (above, size // 2, size // 2), False, recv)

    def hand_over(i, own, size):
        received(ball.at[pl.ds(0, len(groups[i])), pl.ds(0, size), :], yrecv.at[len(GROUPS) + i])
        for off in groups[i]:
            ref = ball.at[blk(*off), pl.ds(own * SIDE * SLICES[0], SIDE * size), :]
            remote(ref, ref, psems, psemr.at[i], {"tp": t + 1 - 2 * own}).start()

    def handed(i, own, size):
        rows = SIDE * SLICES[1 - own]
        received(ball.at[pl.ds(0, len(groups[i])), pl.ds(0, rows), :], psemr.at[i])

    def all_sent(own, size):
        sent(ball.at[pl.ds(0, len(NEAR + ACROSS)), pl.ds(0, size), :], bsend)
        sent(ball.at[pl.ds(0, len(DIAGONAL + FAR)), pl.ds(0, size), :], bsend)
        sent(ball.at[pl.ds(0, FS - 1), pl.ds(0, 3 * size), :], ysend)
        sent(ball.at[pl.ds(0, FS - 1), pl.ds(0, SIDE * size), :], psems)

    def outputs_of(b):
        return jnp.concatenate([ball[b, 256:320, 0:128], ball[b, 256:320, 128:256]], axis=0)

    def project(offs, first=False):
        bs = [blk(*off) for off in offs]
        xs = [x[:, pl.ds(pl.multiple_of(b * 256, 256), 256)] for b in bs]
        cs = [c[:, pl.ds(pl.multiple_of(b * 128, 128), 128)] for b in bs]
        px = dot(
            jnp.concatenate(xs, axis=1), jnp.concatenate([ball[b, 0:256, :] for b in bs], axis=0)
        )
        pc = dot(jnp.concatenate(cs, axis=1), jnp.concatenate([outputs_of(b) for b in bs], axis=0))
        if first:
            xb[...] = px
            cb[...] = pc
        else:
            xb[...] += px
            cb[...] += pc

    by_core(spread_own)
    loaded(wqv, 1)
    loaded(wo, 2)
    wall[f, 0:256, :] = wqv[...].astype(bf16)
    wall[f, 256:384, :] = wo[...].astype(bf16)
    weights.step(0)
    by_core(functools.partial(send_levels, 0))
    by_core(functools.partial(send_levels, 1))
    for s in range(1, 4):
        weights.step(s)
    loaded(x, 3)
    loaded(c, 4)
    project([(0, 0)], first=True)
    by_core(functools.partial(relay_levels, 0))
    by_core(functools.partial(send_levels, 2))
    for g, sem, lo, hi in ((gq, 5, 0, 256), (gv, 6, 256, 512), (go, 7, 512, 1024)):
        loaded(g, sem)
        gt[lo:hi, :] = g[...].T
    by_core(functools.partial(relay_levels, 1))
    by_core(functools.partial(send_levels, 3))
    weights.step(4)
    by_core(functools.partial(hand_over, 0))
    by_core(functools.partial(relay_levels, 2))
    by_core(functools.partial(hand_over, 1))
    weights.step(5)
    by_core(functools.partial(relay_levels, 3))
    weights.step(6)
    by_core(functools.partial(handed, 0))
    project(NEAR[0:2])
    project(NEAR[2:4])
    by_core(functools.partial(hand_over, 2))
    weights.step(7)
    by_core(functools.partial(handed, 1))
    project(ACROSS)
    by_core(functools.partial(hand_over, 3))
    weights.step(8)
    by_core(functools.partial(handed, 2))
    project(DIAGONAL[0:2])
    project(DIAGONAL[2:4])
    weights.step(9)
    by_core(functools.partial(handed, 3))
    project(FAR[0:2])
    project(FAR[2:4])
    project(FAR[4:5])


    def split(a, at):
        hi = a.astype(bf16)
        hl[:, at : at + 128] = hi
        hl[:, at + 128 : at + 256] = (a - hi.astype(f32)).astype(bf16)

    split(xb[:, 0:128], 0)
    split(xb[:, 128:256], 256)
    split(cb[...], 512)
    for at, lo, hi in ((0, 0, 256), (256, 256, 512), (512, 512, 1024)):
        both = dot(gt[lo:hi, :], hl[:, at : at + 256])
        both = (both[:, 0:128] + both[:, 128:256]).astype(bf16)
        for j in range(lo // COLS, hi // COLS):
            psend[j] = both[j * COLS - lo : (j + 1) * COLS - lo, :]

    def grams(js, first=False):
        gq_sum = jnp.zeros((256, 256), f32)
        go_sum = jnp.zeros((128, 128), f32)
        for j in js:
            bqv = ball[j, 0:256, :]
            bo = outputs_of(j)
            gq_sum += dot00(bqv, bqv)
            go_sum += dot00(bo, bo)
        for i, g in enumerate((gq_sum[0:128, 0:128], gq_sum[128:256, 128:256], go_sum)):
            gram[i] = g if first else gram[i] + g

    grams(range(0, 1), first=True)

    def to_peer(src, dst, send, recv, off):
        remote(src, dst, send, recv, {"fs": blk(*off)}).start()

    for off in OTHERS:
        to_peer(psend.at[blk(*off)], precv.at[f], rsend, rrecv, off)
    weights.step(10)
    grams(range(1, FS))
    precv[f] = psend[f]
    loaded(mean, 8)
    loaded(square, 9)
    slab = pl.ds(pl.multiple_of((f // 2) * 128, 128), 128)
    turned[0] = mean[:, slab].T
    turned[1] = square[:, slab].T
    weights.step(11)
    peers = pl.ds(0, FS - 1)
    received(precv.at[peers], rrecv)
    total = precv[0].astype(f32)
    for j in range(1, FS):
        total += precv[j].astype(f32)
    total = total.astype(bf16)
    pall[f] = total

    def moments(p, mean_old, square_old):
        one = beta_first * mean_old + (1.0 - beta_first) * p
        two = beta_second * square_old + (1.0 - beta_second) * p * p
        return one, two, one / jnp.sqrt(two)

    own = pl.ds(pl.multiple_of(lax.rem(f, 2) * COLS, COLS), COLS)
    _, _, own_d = moments(total.astype(f32), turned[0, own, :], turned[1, own, :])
    gd = jnp.dot(
        own_d, gram[jnp.minimum(f // 4, 2)], precision=HIGH, preferred_element_type=f32
    )
    sqf[f] = jnp.broadcast_to(jnp.sum(own_d * gd, keepdims=True), (1, 128))
    for off in OTHERS:
        to_peer(sqf.at[f], sqf.at[f], fsend, frecv, off)
    for off in NEAR + ACROSS:
        to_peer(pall.at[f], pall.at[f], asend, arecv.at[0], off)
    weights.step(12)
    weights.step(13)
    received(sqf.at[peers], frecv)
    squares = sqf[0]
    for j in range(1, FS):
        squares += sqf[j]
    sqs[t] = squares

    for r in range(1, TP):
        remote(sqs.at[t], sqs.at[t], ssend, srecv, {"tp": lax.rem(t + r, TP)}).start()
    received(pall.at[pl.ds(0, len(NEAR + ACROSS))], arecv.at[0])
    upper, lower = pl.ds(0, COLS // 2), pl.ds(COLS // 2, COLS // 2)
    for step in (1, -1, 2):
        for to in (1, -1, 2):
            ref = pall.at[blk(0, step), upper, :]
            to_peer(ref, ref, asend, arecv.at[1], (to, 0))
            ref = pall.at[blk(step, 0), lower, :]
            to_peer(ref, ref, asend, arecv.at[1], (0, to))
    weights.step(14)
    received(pall.at[pl.ds(0, len(DIAGONAL + FAR))], arecv.at[1])
    firsts = [(f1q, 0), (f1q, 128), (f1v, 0), (f1v, 128)] + [(f1o, 128 * i) for i in range(4)]
    seconds = [(f2q, 0), (f2q, 128), (f2v, 0), (f2v, 128)] + [(f2o, 128 * i) for i in range(4)]
    for k in range(8):
        at = slice(128 * k, 128 * k + 128)
        p = jnp.concatenate([pall[2 * k], pall[2 * k + 1]], axis=0).astype(f32).T
        one, two, d[:, at] = moments(p, mean[:, at], square[:, at])
        ref, lo = firsts[k]
        ref[:, lo : lo + 128] = one
        ref, lo = seconds[k]
        ref[:, lo : lo + 128] = two
    hi = d[...].astype(bf16)
    lo = (d[...] - hi.astype(f32)).astype(bf16)
    bqv, bo = ball[f, 0:256, :], outputs_of(f)
    low_q = dot(bqv[:, 0:128], hi[:, 0:256]) + dot(bqv[:, 0:128], lo[:, 0:256])
    low_v = dot(bqv[:, 128:256], hi[:, 256:512]) + dot(bqv[:, 128:256], lo[:, 256:512])
    low_o = dot(bo, hi[:, 512:1024]) + dot(bo, lo[:, 512:1024])
    stq[...] = low_q
    stv[...] = low_v
    sto[...] = low_o
    received(sqs.at[pl.ds(0, TP - 1)], srecv)
    squares = sqs[0]
    for i in range(1, TP):
        squares += sqs[i]
    factor = 1.0 / jnp.sqrt(squares[0:1, 0:1] / (3.0 * MODEL * CELL) + floor_mean)
    dcopy[...] = (-learn_rate * factor * d[...]).astype(bf16)
    stq[...] = -factor * stq[...]
    stv[...] = -factor * stv[...]
    sto[...] = -factor * sto[...]
    for off in OTHERS:
        weights.block(off)
    weights.finish()
    by_core(all_sent)
    sent(psend.at[peers], rsend)
    sent(pall.at[peers], asend)
    sent(sqf.at[peers], fsend)
    sent(sqs.at[pl.ds(0, TP - 1)], ssend)


def finish_kernel(
    wall, ball, dcopy, stq, stv, sto, f1q, f1v, f1o, f2q, f2v, f2o,
    o_stq, o_stv, o_sto, o_q, o_v, o_o, o_f1q, o_f1v, o_f1o, o_f2q, o_f2v, o_f2o,
    cq, cv, co, sem, csem,
):
    plain = [
        pltpu.make_async_copy(src, dst, sem.at[i])
        for i, (src, dst) in enumerate(
            (
                (stq, o_stq), (stv, o_stv), (sto, o_sto), (f1q, o_f1q), (f1v, o_f1v),
                (f1o, o_f1o), (f2q, o_f2q), (f2v, o_f2v), (f2o, o_f2o),
            )
        )
    ]
    for cp in plain:
        cp.start()
    for k in range(FS):
        bo = jnp.concatenate([ball[k, 256:320, 0:128], ball[k, 256:320, 128:256]], axis=0)
        wq = wall[k, 0:256, 0:256].astype(f32)
        cq[k * 256 : k * 256 + 256, :] = (
            wq + dot(ball[k, 0:256, 0:128], dcopy[:, 0:256])
        ).astype(bf16)
        wv = wall[k, 0:256, 256:512].astype(f32)
        cv[k * 256 : k * 256 + 256, :] = (
            wv + dot(ball[k, 0:256, 128:256], dcopy[:, 256:512])
        ).astype(bf16)
        wo = wall[k, 256:384, :].astype(f32)
        co[k * 128 : k * 128 + 128, :] = (wo + dot(bo, dcopy[:, 512:1024])).astype(bf16)
        for i, (src, dst, n) in enumerate(((cq, o_q, 256), (cv, o_v, 256), (co, o_o, 128))):
            cp = pltpu.make_async_copy(
                src.at[pl.ds(k * n, n), :], dst.at[pl.ds(k * n, n), :], csem.at[i]
            )
            cp.start()
    for cp in plain:
        cp.wait()
    for i, (src, dst) in enumerate(((cq, o_q), (cv, o_v), (co, o_o))):
        pltpu.make_async_copy(src, dst, csem.at[i]).wait()


def local(*args):
    tokens = args[0].shape[0]
    any_spec = pl.BlockSpec(memory_space=pl.ANY)
    vmem_spec = pl.BlockSpec(memory_space=pltpu.VMEM)
    steps = [((256, 256), f32), ((256, 256), f32), ((128, 512), f32)]
    news = [((MODEL, 256), bf16), ((MODEL, 256), bf16), ((CELL, 512), bf16)]
    moment = [((128, 256), f32), ((128, 256), f32), ((128, 512), f32)]
    mids = [((FS, W_ROWS, 512), bf16), ((FS, B_ROWS, 256), bf16), ((128, 1024), bf16)]
    mids += steps + moment + moment
    outs = steps + news + moment + moment
    dma = pltpu.SemaphoreType.DMA
    mid = pl.pallas_call(
        gather_kernel,
        out_shape=[pltpu.VMEM(s, t) for s, t in mids],
        in_specs=[any_spec] * 17,
        out_specs=[vmem_spec] * len(mids),
        scratch_shapes=[
            pltpu.VMEM((tokens, MODEL), bf16),
            pltpu.VMEM((tokens, CELL), bf16),
            pltpu.VMEM((tokens, 256), bf16),
            pltpu.VMEM((tokens, 256), bf16),
            pltpu.VMEM((tokens, 512), bf16),
            pltpu.VMEM((256, 512), f32),
            pltpu.VMEM((128, 512), f32),
            pltpu.VMEM((128, 1024), f32),
            pltpu.VMEM((128, 1024), f32),
            pltpu.VMEM((tokens, 256), f32),
            pltpu.VMEM((tokens, 128), f32),
            pltpu.VMEM((1024, tokens), bf16),
            pltpu.VMEM((tokens, 768), bf16),
            pltpu.VMEM((FS, COLS, 128), bf16),
            pltpu.VMEM((FS, COLS, 128), bf16),
            pltpu.VMEM((FS, COLS, 128), bf16),
            pltpu.VMEM((3, 128, 128), f32),
            pltpu.VMEM((2, 128, 128), f32),
            pltpu.VMEM((128, 1024), f32),
            pltpu.VMEM((FS, 1, 128), f32),
            pltpu.VMEM((TP, 1, 128), f32),
            dma((10,)),
            dma, dma((STEPS,)), dma, dma((4,)), dma, dma((4,)), dma, dma((8,)),
            dma, dma, dma, dma((2,)), dma, dma, dma, dma,
        ],
        compiler_params=pltpu.CompilerParams(
            collective_id=0, has_side_effects=True, vmem_limit_bytes=50 * 1024 * 1024
        ),
        name="gather_and_reduce",
    )(*args)
    return tuple(
        pl.pallas_call(
            finish_kernel,
            out_shape=[jax.ShapeDtypeStruct(s, t) for s, t in outs],
            in_specs=[vmem_spec] * len(mids),
            out_specs=[any_spec] * len(outs),
            scratch_shapes=[
                pltpu.VMEM((MODEL, 256), bf16),
                pltpu.VMEM((MODEL, 256), bf16),
                pltpu.VMEM((CELL, 512), bf16),
                dma((9,)),
                dma((3,)),
            ],
            compiler_params=pltpu.CompilerParams(vmem_limit_bytes=12 * 1024 * 1024),
            name="write_copies",
        )(*mid)
    )


def solution(mesh):
    fs, both, tp = P("fs", None), P("fs", "tp"), P(None, "tp")
    in_specs = (fs, fs) + (both,) * 6 + (fs,) * 3 + (tp,) * 6
    out_specs = (both,) * 3 + (tp,) * 9
    return jax.shard_map(local, mesh=mesh, in_specs=in_specs, out_specs=out_specs, check_vma=False)
```

```python
import functools

import jax
import jax.numpy as jnp
from jax import lax
from jax.experimental import pallas as pl
from jax.experimental.pallas import tpu as pltpu
from jax.sharding import PartitionSpec as P

MODEL = 4096
CELL = 2048

beta_first = 0.8
beta_second = 0.9
floor_mean = 0.005
learn_rate = 0.05

f32 = jnp.float32
bf16 = jnp.bfloat16
HIGH = lax.Precision.HIGHEST
SIDE = 4
FS = SIDE * SIDE
TP = 8
B_ROWS = 320
W_ROWS = 384
COLS = 64
SLICES = (32, 48)
W_CUTS = ((0, 96), (96, 96), (192, 96), (288, 96))
NEAR = [(0, 1), (0, -1), (1, 0), (-1, 0)]
ACROSS = [(0, 2), (2, 0)]
DIAGONAL = [(-1, -1), (-1, 1), (1, -1), (1, 1)]
FAR = [(-1, 2), (2, -1), (1, 2), (2, 1), (2, 2)]
GROUPS = (NEAR, ACROSS, DIAGONAL, FAR)
OTHERS = NEAR + ACROSS + DIAGONAL + FAR
MESH = pl.DeviceIdType.MESH


def slot(dz, dx):
    return (dz % SIDE) * SIDE + dx % SIDE


def link_plan(along_x, sign):
    near, far = ((0, 1), (2, 3)) if along_x else ((2, 3), (0, 1))
    which = 0 if sign > 0 else 1

    def at(far_off, near_off):
        return (far_off, near_off) if along_x else (near_off, far_off)

    steps = [(at(0, 0), near[0]), (at(0, 0), near[1]), (at(0, 0), far[0]), (at(0, 0), far[1])]
    steps.append((at(0, -sign), near[which]))
    steps += [(at(-1, 0), far[0]), (at(-1, 0), far[1]), (at(1, 0), far[0]), (at(1, 0), far[1])]
    steps.append((at(0, -sign), far[which]))
    steps += [(at(2, 0), far[0]), (at(2, 0), far[1])]
    steps += [(at(-1, -sign), far[which]), (at(1, -sign), far[which]), (at(2, -sign), far[which])]
    return steps


LINKS = [(True, 1), (True, -1), (False, 1), (False, -1)]
PLANS = [link_plan(*link) for link in LINKS]
STEPS = 15


def dot00(a, b):
    return lax.dot_general(a, b, (((0,), (0,)), ((), ())), preferred_element_type=f32)


def dot(a, b):
    return jnp.dot(a, b, preferred_element_type=f32)


def arrivals():
    got = {}
    for (along_x, sign), plan in zip(LINKS, PLANS):
        for s, (off, piece) in enumerate(plan):
            dest = (off[0], off[1] - sign) if along_x else (off[0] - sign, off[1])
            got[slot(*dest), piece] = s
    return got


ARRIVALS = arrivals()


class Torus:
    def __init__(self, buf, rows, send, recv, blk, neighbour):
        self.buf, self.rows, self.send, self.recv = buf, rows, send, recv
        self.blk, self.neighbour = blk, neighbour
        self.seen = set()

    def copy(self, src, dst, send, recv, link):
        return pltpu.make_async_remote_copy(
            src_ref=src,
            dst_ref=dst,
            send_sem=send,
            recv_sem=recv,
            device_id={"fs": self.neighbour[link]},
            device_id_type=MESH,
        )

    def need(self, off, piece):
        s = ARRIVALS.get((slot(*off), piece))
        if s is None or s in self.seen:
            return
        self.seen.add(s)
        block = self.buf.at[0]
        self.copy(block, block, self.send, self.recv.at[s], 0).wait_recv()

    def step(self, s):
        for link in range(len(LINKS)):
            off, piece = PLANS[link][s]
            self.need(off, piece)
            start, size = self.rows[piece]
            ref = self.buf.at[self.blk(*off), pl.ds(start, size), :]
            self.copy(ref, ref, self.send, self.recv.at[s], link).start()

    def block(self, off):
        for piece in range(4):
            self.need(off, piece)

    def finish(self):
        sent = self.buf.at[pl.ds(0, STEPS)]
        self.copy(sent, sent, self.send, self.recv.at[0], 0).wait_send()


def gather_kernel(
    x_h, c_h, gq_h, gv_h, go_h, wq_h, wv_h, wo_h, bq_h, bv_h, bo_h,
    mq_h, mv_h, mo_h, sq_h, sv_h, so_h,
    wall, ball, dcopy, stq, stv, sto, f1q, f1v, f1o, f2q, f2v, f2o,
    x, c, gq, gv, go, wqv, wo, mean, square,
    xb, cb, gt, hl, psend, precv, pall, gram, turned, d, sqf, sqs,
    lsem, wsend, wrecv, bsend, brecv, psems, psemr, ysend, yrecv, rsend, rrecv, asend, arecv,
    fsend, frecv, ssend, srecv,
):
    f = lax.axis_index("fs")
    t = lax.axis_index("tp")
    z, xx = f // SIDE, lax.rem(f, SIDE)
    core = lax.rem(t, 2)

    def blk(dz, dx):
        return lax.rem(z + (dz % SIDE), SIDE) * SIDE + lax.rem(xx + (dx % SIDE), SIDE)

    barrier = pltpu.get_barrier_semaphore()
    for off in NEAR + ACROSS:
        pl.semaphore_signal(barrier, inc=1, device_id={"fs": blk(*off)}, device_id_type=MESH)
    for peer in (lax.rem(t + 2, TP), lax.rem(t + TP - 2, TP), t + 1 - 2 * core):
        pl.semaphore_signal(barrier, inc=1, device_id={"tp": peer}, device_id_type=MESH)

    def load(src, dst, sem):
        pltpu.make_async_copy(src, dst, lsem.at[sem]).start()

    def loaded(ref, sem):
        pltpu.make_async_copy(ref, ref, lsem.at[sem]).wait()

    load(bq_h, ball.at[f, pl.ds(0, 256), pl.ds(0, 128)], 0)
    load(bv_h, ball.at[f, pl.ds(0, 256), pl.ds(128, 128)], 0)
    load(bo_h.at[pl.ds(0, 64), :], ball.at[f, pl.ds(256, 64), pl.ds(0, 128)], 0)
    load(bo_h.at[pl.ds(64, 64), :], ball.at[f, pl.ds(256, 64), pl.ds(128, 128)], 0)
    load(wq_h, wqv.at[:, pl.ds(0, 256)], 1)
    load(wv_h, wqv.at[:, pl.ds(256, 256)], 1)
    load(wo_h, wo, 2)
    load(x_h, x, 3)
    load(c_h, c, 4)
    load(gq_h, gq, 5)
    load(gv_h, gv, 6)
    load(go_h, go, 7)
    for at, mean_in, square_in in ((0, mq_h, sq_h), (256, mv_h, sv_h), (512, mo_h, so_h)):
        cols = pl.ds(at, mean_in.shape[1])
        load(mean_in, mean.at[:, cols], 8)
        load(square_in, square.at[:, cols], 9)

    loaded(ball.at[f], 0)
    pl.semaphore_wait(barrier, len(NEAR + ACROSS) + 3)

    neighbour = [blk(0, 1), blk(0, -1), blk(1, 0), blk(-1, 0)]
    weights = Torus(wall, W_CUTS, wsend, wrecv, blk, neighbour)
    y = t // 2
    above, below = lax.rem(y + 1, SIDE), lax.rem(y + SIDE - 1, SIDE)
    groups = GROUPS

    def by_core(fn):
        for own in range(2):
            pl.when(core == own)(functools.partial(fn, own, SLICES[own]))

    def slice_rows(own, level, start, size):
        at = own * SIDE * SLICES[0] + level * SLICES[own] + start
        return pl.ds(pl.multiple_of(at, 8), size)

    def remote(src, dst, send, recv, device_id):
        return pltpu.make_async_remote_copy(
            src_ref=src,
            dst_ref=dst,
            send_sem=send,
            recv_sem=recv,
            device_id=device_id,
            device_id_type=MESH,
        )

    def received(ref, recv):
        remote(ref, ref, recv, recv, {"fs": neighbour[0]}).wait_recv()

    def sent(ref, send):
        remote(ref, ref, send, send, {"fs": neighbour[0]}).wait_send()

    def group_of(off):
        return [slot(*off) in [slot(*o) for o in g] for g in groups].index(True)

    def in_plane(own, off, start, size, to):
        arriving = (off[0] - to[0], off[1] - to[1])
        ref = ball.at[blk(*off), slice_rows(own, y, start, size), :]
        remote(ref, ref, bsend, brecv.at[group_of(arriving)], {"fs": blk(*to)}).start()

    def spread_own(own, size):
        for off in NEAR + ACROSS:
            in_plane(own, (0, 0), 0, size, off)

    def turn(blocks, own, size):
        for dz, dx in blocks:
            peers = [(1, 0), (-1, 0), (2, 0)] if dz == 0 else [(0, 1), (0, -1), (0, 2)]
            for to in peers:
                in_plane(own, (dz, dx), 0 if dz == 0 else size // 2, size // 2, to)

    def level(own, off, rows, up, recv):
        ref = ball.at[blk(*off), slice_rows(own, *rows), :]
        remote(ref, ref, ysend, recv, {"tp": (above if up else below) * 2 + core}).start()

    def send_levels(i, own, size):
        received(ball.at[pl.ds(0, len(groups[i])), pl.ds(0, size), :], brecv.at[i])
        for off in groups[i]:
            level(own, off, (y, 0, size), True, yrecv.at[i])
            level(own, off, (y, 0, size), False, yrecv.at[i])
        if i < 2:
            turn(groups[i], own, size)

    def relay_levels(i, own, size):
        received(ball.at[pl.ds(0, len(groups[i])), pl.ds(0, 2 * size), :], yrecv.at[i])
        for off in groups[i]:
            recv = yrecv.at[len(GROUPS) + i]
            level(own, off, (below, 0, size // 2), True, recv)
            level(own, off, (above, size // 2, size // 2), False, recv)

    def hand_over(i, own, size):
        received(ball.at[pl.ds(0, len(groups[i])), pl.ds(0, size), :], yrecv.at[len(GROUPS) + i])
        for off in groups[i]:
            ref = ball.at[blk(*off), pl.ds(own * SIDE * SLICES[0], SIDE * size), :]
            remote(ref, ref, psems, psemr.at[i], {"tp": t + 1 - 2 * own}).start()

    def handed(i, own, size):
        rows = SIDE * SLICES[1 - own]
        received(ball.at[pl.ds(0, len(groups[i])), pl.ds(0, rows), :], psemr.at[i])

    def all_sent(own, size):
        sent(ball.at[pl.ds(0, len(NEAR + ACROSS)), pl.ds(0, size), :], bsend)
        sent(ball.at[pl.ds(0, len(DIAGONAL + FAR)), pl.ds(0, size), :], bsend)
        sent(ball.at[pl.ds(0, FS - 1), pl.ds(0, 3 * size), :], ysend)
        sent(ball.at[pl.ds(0, FS - 1), pl.ds(0, SIDE * size), :], psems)

    def outputs_of(b):
        return jnp.concatenate([ball[b, 256:320, 0:128], ball[b, 256:320, 128:256]], axis=0)

    def project(offs, first=False):
        bs = [blk(*off) for off in offs]
        xs = [x[:, pl.ds(pl.multiple_of(b * 256, 256), 256)] for b in bs]
        cs = [c[:, pl.ds(pl.multiple_of(b * 128, 128), 128)] for b in bs]
        px = dot(
            jnp.concatenate(xs, axis=1), jnp.concatenate([ball[b, 0:256, :] for b in bs], axis=0)
        )
        pc = dot(jnp.concatenate(cs, axis=1), jnp.concatenate([outputs_of(b) for b in bs], axis=0))
        if first:
            xb[...] = px
            cb[...] = pc
        else:
            xb[...] += px
            cb[...] += pc

    by_core(spread_own)
    loaded(wqv, 1)
    loaded(wo, 2)
    wall[f, 0:256, :] = wqv[...].astype(bf16)
    wall[f, 256:384, :] = wo[...].astype(bf16)
    weights.step(0)
    by_core(functools.partial(send_levels, 0))
    by_core(functools.partial(send_levels, 1))
    for s in range(1, 4):
        weights.step(s)
    loaded(x, 3)
    loaded(c, 4)
    project([(0, 0)], first=True)
    by_core(functools.partial(relay_levels, 0))
    by_core(functools.partial(send_levels, 2))
    for g, sem, lo, hi in ((gq, 5, 0, 256), (gv, 6, 256, 512), (go, 7, 512, 1024)):
        loaded(g, sem)
        gt[lo:hi, :] = g[...].T
    by_core(functools.partial(relay_levels, 1))
    by_core(functools.partial(send_levels, 3))
    weights.step(4)
    by_core(functools.partial(hand_over, 0))
    by_core(functools.partial(relay_levels, 2))
    by_core(functools.partial(hand_over, 1))
    weights.step(5)
    by_core(functools.partial(relay_levels, 3))
    weights.step(6)
    by_core(functools.partial(handed, 0))
    project(NEAR[0:2])
    project(NEAR[2:4])
    by_core(functools.partial(hand_over, 2))
    weights.step(7)
    by_core(functools.partial(handed, 1))
    project(ACROSS)
    by_core(functools.partial(hand_over, 3))
    weights.step(8)
    by_core(functools.partial(handed, 2))
    project(DIAGONAL[0:2])
    project(DIAGONAL[2:4])
    weights.step(9)
    by_core(functools.partial(handed, 3))
    project(FAR[0:2])
    project(FAR[2:4])
    project(FAR[4:5])


    def split(a, at):
        hi = a.astype(bf16)
        hl[:, at : at + 128] = hi
        hl[:, at + 128 : at + 256] = (a - hi.astype(f32)).astype(bf16)

    split(xb[:, 0:128], 0)
    split(xb[:, 128:256], 256)
    split(cb[...], 512)
    for at, lo, hi in ((0, 0, 256), (256, 256, 512), (512, 512, 1024)):
        both = dot(gt[lo:hi, :], hl[:, at : at + 256])
        both = (both[:, 0:128] + both[:, 128:256]).astype(bf16)
        for j in range(lo // COLS, hi // COLS):
            psend[j] = both[j * COLS - lo : (j + 1) * COLS - lo, :]

    def grams(js, first=False):
        gq_sum = jnp.zeros((256, 256), f32)
        go_sum = jnp.zeros((128, 128), f32)
        for j in js:
            bqv = ball[j, 0:256, :]
            bo = outputs_of(j)
            gq_sum += dot00(bqv, bqv)
            go_sum += dot00(bo, bo)
        for i, g in enumerate((gq_sum[0:128, 0:128], gq_sum[128:256, 128:256], go_sum)):
            gram[i] = g if first else gram[i] + g

    grams(range(0, 1), first=True)

    def to_peer(src, dst, send, recv, off):
        remote(src, dst, send, recv, {"fs": blk(*off)}).start()

    for off in OTHERS:
        to_peer(psend.at[blk(*off)], precv.at[f], rsend, rrecv, off)
    weights.step(10)
    grams(range(1, FS))
    precv[f] = psend[f]
    loaded(mean, 8)
    loaded(square, 9)
    slab = pl.ds(pl.multiple_of((f // 2) * 128, 128), 128)
    turned[0] = mean[:, slab].T
    turned[1] = square[:, slab].T
    weights.step(11)
    peers = pl.ds(0, FS - 1)
    received(precv.at[peers], rrecv)
    total = precv[0].astype(f32)
    for j in range(1, FS):
        total += precv[j].astype(f32)
    total = total.astype(bf16)
    pall[f] = total

    def moments(p, mean_old, square_old):
        one = beta_first * mean_old + (1.0 - beta_first) * p
        two = beta_second * square_old + (1.0 - beta_second) * p * p
        return one, two, one / jnp.sqrt(two)

    own = pl.ds(pl.multiple_of(lax.rem(f, 2) * COLS, COLS), COLS)
    _, _, own_d = moments(total.astype(f32), turned[0, own, :], turned[1, own, :])
    gd = jnp.dot(
        own_d, gram[jnp.minimum(f // 4, 2)], precision=HIGH, preferred_element_type=f32
    )
    sqf[f] = jnp.broadcast_to(jnp.sum(own_d * gd, keepdims=True), (1, 128))
    for off in OTHERS:
        to_peer(sqf.at[f], sqf.at[f], fsend, frecv, off)
    for off in NEAR + ACROSS:
        to_peer(pall.at[f], pall.at[f], asend, arecv.at[0], off)
    weights.step(12)
    weights.step(13)
    received(sqf.at[peers], frecv)
    squares = sqf[0]
    for j in range(1, FS):
        squares += sqf[j]
    sqs[t] = squares

    for r in range(1, TP):
        remote(sqs.at[t], sqs.at[t], ssend, srecv, {"tp": lax.rem(t + r, TP)}).start()
    received(pall.at[pl.ds(0, len(NEAR + ACROSS))], arecv.at[0])
    upper, lower = pl.ds(0, COLS // 2), pl.ds(COLS // 2, COLS // 2)
    for step in (1, -1, 2):
        for to in (1, -1, 2):
            ref = pall.at[blk(0, step), upper, :]
            to_peer(ref, ref, asend, arecv.at[1], (to, 0))
            ref = pall.at[blk(step, 0), lower, :]
            to_peer(ref, ref, asend, arecv.at[1], (0, to))
    weights.step(14)
    received(pall.at[pl.ds(0, len(DIAGONAL + FAR))], arecv.at[1])
    firsts = [(f1q, 0), (f1q, 128), (f1v, 0), (f1v, 128)] + [(f1o, 128 * i) for i in range(4)]
    seconds = [(f2q, 0), (f2q, 128), (f2v, 0), (f2v, 128)] + [(f2o, 128 * i) for i in range(4)]
    for k in range(8):
        at = slice(128 * k, 128 * k + 128)
        p = jnp.concatenate([pall[2 * k], pall[2 * k + 1]], axis=0).astype(f32).T
        one, two, d[:, at] = moments(p, mean[:, at], square[:, at])
        ref, lo = firsts[k]
        ref[:, lo : lo + 128] = one
        ref, lo = seconds[k]
        ref[:, lo : lo + 128] = two
    hi = d[...].astype(bf16)
    lo = (d[...] - hi.astype(f32)).astype(bf16)
    bqv, bo = ball[f, 0:256, :], outputs_of(f)
    low_q = dot(bqv[:, 0:128], hi[:, 0:256]) + dot(bqv[:, 0:128], lo[:, 0:256])
    low_v = dot(bqv[:, 128:256], hi[:, 256:512]) + dot(bqv[:, 128:256], lo[:, 256:512])
    low_o = dot(bo, hi[:, 512:1024]) + dot(bo, lo[:, 512:1024])
    stq[...] = low_q
    stv[...] = low_v
    sto[...] = low_o
    received(sqs.at[pl.ds(0, TP - 1)], srecv)
    squares = sqs[0]
    for i in range(1, TP):
        squares += sqs[i]
    factor = 1.0 / jnp.sqrt(squares[0:1, 0:1] / (3.0 * MODEL * CELL) + floor_mean)
    dcopy[...] = (-learn_rate * factor * d[...]).astype(bf16)
    stq[...] = -factor * stq[...]
    stv[...] = -factor * stv[...]
    sto[...] = -factor * sto[...]
    for off in OTHERS:
        weights.block(off)
    weights.finish()
    by_core(all_sent)
    sent(psend.at[peers], rsend)
    sent(pall.at[peers], asend)
    sent(sqf.at[peers], fsend)
    sent(sqs.at[pl.ds(0, TP - 1)], ssend)


def finish_kernel(
    wall, ball, dcopy, stq, stv, sto, f1q, f1v, f1o, f2q, f2v, f2o,
    o_stq, o_stv, o_sto, o_q, o_v, o_o, o_f1q, o_f1v, o_f1o, o_f2q, o_f2v, o_f2o,
    cq, cv, co, sem, csem,
):
    plain = [
        pltpu.make_async_copy(src, dst, sem.at[i])
        for i, (src, dst) in enumerate(
            (
                (stq, o_stq), (stv, o_stv), (sto, o_sto), (f1q, o_f1q), (f1v, o_f1v),
                (f1o, o_f1o), (f2q, o_f2q), (f2v, o_f2v), (f2o, o_f2o),
            )
        )
    ]
    for cp in plain:
        cp.start()
    for k in range(FS):
        bo = jnp.concatenate([ball[k, 256:320, 0:128], ball[k, 256:320, 128:256]], axis=0)
        wq = wall[k, 0:256, 0:256].astype(f32)
        cq[k * 256 : k * 256 + 256, :] = (
            wq + dot(ball[k, 0:256, 0:128], dcopy[:, 0:256])
        ).astype(bf16)
        wv = wall[k, 0:256, 256:512].astype(f32)
        cv[k * 256 : k * 256 + 256, :] = (
            wv + dot(ball[k, 0:256, 128:256], dcopy[:, 256:512])
        ).astype(bf16)
        wo = wall[k, 256:384, :].astype(f32)
        co[k * 128 : k * 128 + 128, :] = (wo + dot(bo, dcopy[:, 512:1024])).astype(bf16)
        for i, (src, dst, n) in enumerate(((cq, o_q, 256), (cv, o_v, 256), (co, o_o, 128))):
            cp = pltpu.make_async_copy(
                src.at[pl.ds(k * n, n), :], dst.at[pl.ds(k * n, n), :], csem.at[i]
            )
            cp.start()
    for cp in plain:
        cp.wait()
    for i, (src, dst) in enumerate(((cq, o_q), (cv, o_v), (co, o_o))):
        pltpu.make_async_copy(src, dst, csem.at[i]).wait()


def local(*args):
    tokens = args[0].shape[0]
    any_spec = pl.BlockSpec(memory_space=pl.ANY)
    vmem_spec = pl.BlockSpec(memory_space=pltpu.VMEM)
    steps = [((256, 256), f32), ((256, 256), f32), ((128, 512), f32)]
    news = [((MODEL, 256), bf16), ((MODEL, 256), bf16), ((CELL, 512), bf16)]
    moment = [((128, 256), f32), ((128, 256), f32), ((128, 512), f32)]
    mids = [((FS, W_ROWS, 512), bf16), ((FS, B_ROWS, 256), bf16), ((128, 1024), bf16)]
    mids += steps + moment + moment
    outs = steps + news + moment + moment
    dma = pltpu.SemaphoreType.DMA
    mid = pl.pallas_call(
        gather_kernel,
        out_shape=[pltpu.VMEM(s, t) for s, t in mids],
        in_specs=[any_spec] * 17,
        out_specs=[vmem_spec] * len(mids),
        scratch_shapes=[
            pltpu.VMEM((tokens, MODEL), bf16),
            pltpu.VMEM((tokens, CELL), bf16),
            pltpu.VMEM((tokens, 256), bf16),
            pltpu.VMEM((tokens, 256), bf16),
            pltpu.VMEM((tokens, 512), bf16),
            pltpu.VMEM((256, 512), f32),
            pltpu.VMEM((128, 512), f32),
            pltpu.VMEM((128, 1024), f32),
            pltpu.VMEM((128, 1024), f32),
            pltpu.VMEM((tokens, 256), f32),
            pltpu.VMEM((tokens, 128), f32),
            pltpu.VMEM((1024, tokens), bf16),
            pltpu.VMEM((tokens, 768), bf16),
            pltpu.VMEM((FS, COLS, 128), bf16),
            pltpu.VMEM((FS, COLS, 128), bf16),
            pltpu.VMEM((FS, COLS, 128), bf16),
            pltpu.VMEM((3, 128, 128), f32),
            pltpu.VMEM((2, 128, 128), f32),
            pltpu.VMEM((128, 1024), f32),
            pltpu.VMEM((FS, 1, 128), f32),
            pltpu.VMEM((TP, 1, 128), f32),
            dma((10,)),
            dma, dma((STEPS,)), dma, dma((4,)), dma, dma((4,)), dma, dma((8,)),
            dma, dma, dma, dma((2,)), dma, dma, dma, dma,
        ],
        compiler_params=pltpu.CompilerParams(
            collective_id=0, has_side_effects=True, vmem_limit_bytes=50 * 1024 * 1024
        ),
        name="gather_and_reduce",
    )(*args)
    return tuple(
        pl.pallas_call(
            finish_kernel,
            out_shape=[jax.ShapeDtypeStruct(s, t) for s, t in outs],
            in_specs=[vmem_spec] * len(mids),
            out_specs=[any_spec] * len(outs),
            scratch_shapes=[
                pltpu.VMEM((MODEL, 256), bf16),
                pltpu.VMEM((MODEL, 256), bf16),
                pltpu.VMEM((CELL, 512), bf16),
                dma((9,)),
                dma((3,)),
            ],
            compiler_params=pltpu.CompilerParams(vmem_limit_bytes=12 * 1024 * 1024),
            name="write_copies",
        )(*mid)
    )


def solution(mesh):
    fs, both, tp = P("fs", None), P("fs", "tp"), P(None, "tp")
    in_specs = (fs, fs) + (both,) * 6 + (fs,) * 3 + (tp,) * 6
    out_specs = (both,) * 3 + (tp,) * 9
    return jax.shard_map(local, mesh=mesh, in_specs=in_specs, out_specs=out_specs, check_vma=False)
```

```python
import functools

import jax
import jax.numpy as jnp
from jax import lax
from jax.experimental import pallas as pl
from jax.experimental.pallas import tpu as pltpu
from jax.sharding import PartitionSpec as P

MODEL = 4096
CELL = 2048

beta_first = 0.8
beta_second = 0.9
floor_mean = 0.005
learn_rate = 0.05

f32 = jnp.float32
bf16 = jnp.bfloat16
HIGH = lax.Precision.HIGHEST
SIDE = 4
FS = SIDE * SIDE
TP = 8
B_ROWS = 320
W_ROWS = 384
COLS = 64
SLICES = (32, 48)
W_CUTS = ((0, 96), (96, 96), (192, 96), (288, 96))
NEAR = [(0, 1), (0, -1), (1, 0), (-1, 0)]
ACROSS = [(0, 2), (2, 0)]
DIAGONAL = [(-1, -1), (-1, 1), (1, -1), (1, 1)]
FAR = [(-1, 2), (2, -1), (1, 2), (2, 1), (2, 2)]
GROUPS = (NEAR, ACROSS, DIAGONAL, FAR)
OTHERS = NEAR + ACROSS + DIAGONAL + FAR
MESH = pl.DeviceIdType.MESH


def slot(dz, dx):
    return (dz % SIDE) * SIDE + dx % SIDE


def link_plan(along_x, sign):
    near, far = ((0, 1), (2, 3)) if along_x else ((2, 3), (0, 1))
    which = 0 if sign > 0 else 1

    def at(far_off, near_off):
        return (far_off, near_off) if along_x else (near_off, far_off)

    steps = [(at(0, 0), near[0]), (at(0, 0), near[1]), (at(0, 0), far[0]), (at(0, 0), far[1])]
    steps.append((at(0, -sign), near[which]))
    steps += [(at(-1, 0), far[0]), (at(-1, 0), far[1]), (at(1, 0), far[0]), (at(1, 0), far[1])]
    steps.append((at(0, -sign), far[which]))
    steps += [(at(2, 0), far[0]), (at(2, 0), far[1])]
    steps += [(at(-1, -sign), far[which]), (at(1, -sign), far[which]), (at(2, -sign), far[which])]
    return steps


LINKS = [(True, 1), (True, -1), (False, 1), (False, -1)]
PLANS = [link_plan(*link) for link in LINKS]
STEPS = 15


def dot00(a, b):
    return lax.dot_general(a, b, (((0,), (0,)), ((), ())), preferred_element_type=f32)


def dot(a, b):
    return jnp.dot(a, b, preferred_element_type=f32)


def arrivals():
    got = {}
    for (along_x, sign), plan in zip(LINKS, PLANS):
        for s, (off, piece) in enumerate(plan):
            dest = (off[0], off[1] - sign) if along_x else (off[0] - sign, off[1])
            got[slot(*dest), piece] = s
    return got


ARRIVALS = arrivals()


class Torus:
    def __init__(self, buf, rows, send, recv, blk, neighbour):
        self.buf, self.rows, self.send, self.recv = buf, rows, send, recv
        self.blk, self.neighbour = blk, neighbour
        self.seen = set()

    def copy(self, src, dst, send, recv, link):
        return pltpu.make_async_remote_copy(
            src_ref=src,
            dst_ref=dst,
            send_sem=send,
            recv_sem=recv,
            device_id={"fs": self.neighbour[link]},
            device_id_type=MESH,
        )

    def need(self, off, piece):
        s = ARRIVALS.get((slot(*off), piece))
        if s is None or s in self.seen:
            return
        self.seen.add(s)
        block = self.buf.at[0]
        self.copy(block, block, self.send, self.recv.at[s], 0).wait_recv()

    def step(self, s):
        for link in range(len(LINKS)):
            off, piece = PLANS[link][s]
            self.need(off, piece)
            start, size = self.rows[piece]
            ref = self.buf.at[self.blk(*off), pl.ds(start, size), :]
            self.copy(ref, ref, self.send, self.recv.at[s], link).start()

    def block(self, off):
        for piece in range(4):
            self.need(off, piece)

    def finish(self):
        sent = self.buf.at[pl.ds(0, STEPS)]
        self.copy(sent, sent, self.send, self.recv.at[0], 0).wait_send()


def gather_kernel(
    x_h, c_h, gq_h, gv_h, go_h, wq_h, wv_h, wo_h, bq_h, bv_h, bo_h,
    mq_h, mv_h, mo_h, sq_h, sv_h, so_h,
    wall, ball, dcopy, stq, stv, sto, f1q, f1v, f1o, f2q, f2v, f2o,
    x, c, gq, gv, go, wqv, wo, mean, square,
    xb, cb, gt, hl, psend, precv, pall, gram, turned, d, sqf, sqs,
    lsem, wsend, wrecv, bsend, brecv, psems, psemr, ysend, yrecv, rsend, rrecv, asend, arecv,
    fsend, frecv, ssend, srecv, entered,
):
    f = lax.axis_index("fs")
    t = lax.axis_index("tp")
    z, xx = f // SIDE, lax.rem(f, SIDE)
    core = lax.rem(t, 2)

    def blk(dz, dx):
        return lax.rem(z + (dz % SIDE), SIDE) * SIDE + lax.rem(xx + (dx % SIDE), SIDE)

    barrier = pltpu.get_barrier_semaphore()
    for off in ACROSS + NEAR:
        pl.semaphore_signal(barrier, inc=1, device_id={"fs": blk(*off)}, device_id_type=MESH)
    for peer in (lax.rem(t + 2, TP), lax.rem(t + TP - 2, TP)):
        pl.semaphore_signal(barrier, inc=1, device_id={"tp": peer}, device_id_type=MESH)

    @pl.when(core == 0)
    def _():
        pl.semaphore_signal(barrier, inc=1, device_id={"tp": t + 1}, device_id_type=MESH)


    def load(src, dst, sem):
        pltpu.make_async_copy(src, dst, lsem.at[sem]).start()

    def loaded(ref, sem):
        pltpu.make_async_copy(ref, ref, lsem.at[sem]).wait()

    load(bq_h, ball.at[f, pl.ds(0, 256), pl.ds(0, 128)], 0)
    load(bv_h, ball.at[f, pl.ds(0, 256), pl.ds(128, 128)], 0)
    load(bo_h.at[pl.ds(0, 64), :], ball.at[f, pl.ds(256, 64), pl.ds(0, 128)], 0)
    load(bo_h.at[pl.ds(64, 64), :], ball.at[f, pl.ds(256, 64), pl.ds(128, 128)], 0)
    load(wq_h, wqv.at[:, pl.ds(0, 256)], 1)
    load(wv_h, wqv.at[:, pl.ds(256, 256)], 1)
    load(wo_h, wo, 2)
    load(x_h, x, 3)
    load(c_h, c, 4)
    load(gq_h, gq, 5)
    load(gv_h, gv, 6)
    load(go_h, go, 7)
    for at, mean_in, square_in in ((0, mq_h, sq_h), (256, mv_h, sv_h), (512, mo_h, so_h)):
        cols = pl.ds(at, mean_in.shape[1])
        load(mean_in, mean.at[:, cols], 8)
        load(square_in, square.at[:, cols], 9)

    loaded(ball.at[f], 0)
    pl.semaphore_wait(barrier, len(NEAR + ACROSS) + 2 + core)

    @pl.when(core == 1)
    def _():
        pl.semaphore_signal(entered, inc=1, device_id={"tp": t - 1}, device_id_type=MESH)


    neighbour = [blk(0, 1), blk(0, -1), blk(1, 0), blk(-1, 0)]
    weights = Torus(wall, W_CUTS, wsend, wrecv, blk, neighbour)
    y = t // 2
    above, below = lax.rem(y + 1, SIDE), lax.rem(y + SIDE - 1, SIDE)
    groups = GROUPS

    def by_core(fn):
        for own in range(2):
            pl.when(core == own)(functools.partial(fn, own, SLICES[own]))

    def slice_rows(own, level, start, size):
        at = own * SIDE * SLICES[0] + level * SLICES[own] + start
        return pl.ds(pl.multiple_of(at, 8), size)

    def remote(src, dst, send, recv, device_id):
        return pltpu.make_async_remote_copy(
            src_ref=src,
            dst_ref=dst,
            send_sem=send,
            recv_sem=recv,
            device_id=device_id,
            device_id_type=MESH,
        )

    def received(ref, recv):
        remote(ref, ref, recv, recv, {"fs": neighbour[0]}).wait_recv()

    def sent(ref, send):
        remote(ref, ref, send, send, {"fs": neighbour[0]}).wait_send()

    def group_of(off):
        return [slot(*off) in [slot(*o) for o in g] for g in groups].index(True)

    def in_plane(own, off, start, size, to):
        arriving = (off[0] - to[0], off[1] - to[1])
        ref = ball.at[blk(*off), slice_rows(own, y, start, size), :]
        remote(ref, ref, bsend, brecv.at[group_of(arriving)], {"fs": blk(*to)}).start()

    def spread_own(own, size):
        for off in NEAR + ACROSS:
            in_plane(own, (0, 0), 0, size, off)

    def turn(blocks, own, size):
        for dz, dx in blocks:
            peers = [(1, 0), (-1, 0), (2, 0)] if dz == 0 else [(0, 1), (0, -1), (0, 2)]
            for to in peers:
                in_plane(own, (dz, dx), 0 if dz == 0 else size // 2, size // 2, to)

    def level(own, off, rows, up, recv):
        ref = ball.at[blk(*off), slice_rows(own, *rows), :]
        remote(ref, ref, ysend, recv, {"tp": (above if up else below) * 2 + core}).start()

    def send_levels(i, own, size):
        received(ball.at[pl.ds(0, len(groups[i])), pl.ds(0, size), :], brecv.at[i])
        for off in groups[i]:
            level(own, off, (y, 0, size), True, yrecv.at[i])
            level(own, off, (y, 0, size), False, yrecv.at[i])
        if i < 2:
            turn(groups[i], own, size)

    def relay_levels(i, own, size):
        received(ball.at[pl.ds(0, len(groups[i])), pl.ds(0, 2 * size), :], yrecv.at[i])
        for off in groups[i]:
            recv = yrecv.at[len(GROUPS) + i]
            level(own, off, (below, 0, size // 2), True, recv)
            level(own, off, (above, size // 2, size // 2), False, recv)

    def hand_over(i, own, size):
        received(ball.at[pl.ds(0, len(groups[i])), pl.ds(0, size), :], yrecv.at[len(GROUPS) + i])
        for off in groups[i]:
            ref = ball.at[blk(*off), pl.ds(own * SIDE * SLICES[0], SIDE * size), :]
            remote(ref, ref, psems, psemr.at[i], {"tp": t + 1 - 2 * own}).start()

    def handed(i, own, size):
        rows = SIDE * SLICES[1 - own]
        received(ball.at[pl.ds(0, len(groups[i])), pl.ds(0, rows), :], psemr.at[i])

    def all_sent(own, size):
        sent(ball.at[pl.ds(0, len(NEAR + ACROSS)), pl.ds(0, size), :], bsend)
        sent(ball.at[pl.ds(0, len(DIAGONAL + FAR)), pl.ds(0, size), :], bsend)
        sent(ball.at[pl.ds(0, FS - 1), pl.ds(0, 3 * size), :], ysend)
        sent(ball.at[pl.ds(0, FS - 1), pl.ds(0, SIDE * size), :], psems)

    def outputs_of(b):
        return jnp.concatenate([ball[b, 256:320, 0:128], ball[b, 256:320, 128:256]], axis=0)

    def project(offs, first=False):
        bs = [blk(*off) for off in offs]
        xs = [x[:, pl.ds(pl.multiple_of(b * 256, 256), 256)] for b in bs]
        cs = [c[:, pl.ds(pl.multiple_of(b * 128, 128), 128)] for b in bs]
        px = dot(
            jnp.concatenate(xs, axis=1), jnp.concatenate([ball[b, 0:256, :] for b in bs], axis=0)
        )
        pc = dot(jnp.concatenate(cs, axis=1), jnp.concatenate([outputs_of(b) for b in bs], axis=0))
        if first:
            xb[...] = px
            cb[...] = pc
        else:
            xb[...] += px
            cb[...] += pc

    by_core(spread_own)
    loaded(wqv, 1)
    loaded(wo, 2)
    wall[f, 0:256, :] = wqv[...].astype(bf16)
    wall[f, 256:384, :] = wo[...].astype(bf16)
    weights.step(0)
    by_core(functools.partial(send_levels, 0))
    by_core(functools.partial(send_levels, 1))
    for s in range(1, 4):
        weights.step(s)
    loaded(x, 3)
    loaded(c, 4)
    project([(0, 0)], first=True)
    by_core(functools.partial(relay_levels, 0))
    by_core(functools.partial(send_levels, 2))
    for g, sem, lo, hi in ((gq, 5, 0, 256), (gv, 6, 256, 512), (go, 7, 512, 1024)):
        loaded(g, sem)
        gt[lo:hi, :] = g[...].T
    by_core(functools.partial(relay_levels, 1))
    by_core(functools.partial(send_levels, 3))
    weights.step(4)
    @pl.when(core == 0)
    def _():
        pl.semaphore_wait(entered, 1)

    by_core(functools.partial(hand_over, 0))
    by_core(functools.partial(relay_levels, 2))
    weights.step(5)
    by_core(functools.partial(hand_over, 1))
    by_core(functools.partial(relay_levels, 3))
    weights.step(6)
    by_core(functools.partial(handed, 0))
    project(NEAR[0:2])
    project(NEAR[2:4])
    by_core(functools.partial(hand_over, 2))
    weights.step(7)
    by_core(functools.partial(handed, 1))
    project(ACROSS)
    by_core(functools.partial(hand_over, 3))
    weights.step(8)
    by_core(functools.partial(handed, 2))
    project(DIAGONAL[0:2])
    project(DIAGONAL[2:4])
    weights.step(9)
    by_core(functools.partial(handed, 3))
    project(FAR[0:2])
    project(FAR[2:4])
    project(FAR[4:5])


    def split(a, at):
        hi = a.astype(bf16)
        hl[:, at : at + 128] = hi
        hl[:, at + 128 : at + 256] = (a - hi.astype(f32)).astype(bf16)

    split(xb[:, 0:128], 0)
    split(xb[:, 128:256], 256)
    split(cb[...], 512)
    for at, lo, hi in ((0, 0, 256), (256, 256, 512), (512, 512, 1024)):
        both = dot(gt[lo:hi, :], hl[:, at : at + 256])
        both = (both[:, 0:128] + both[:, 128:256]).astype(bf16)
        for j in range(lo // COLS, hi // COLS):
            psend[j] = both[j * COLS - lo : (j + 1) * COLS - lo, :]

    def grams(js, first=False):
        gq_sum = jnp.zeros((256, 256), f32)
        go_sum = jnp.zeros((128, 128), f32)
        for j in js:
            bqv = ball[j, 0:256, :]
            bo = outputs_of(j)
            gq_sum += dot00(bqv, bqv)
            go_sum += dot00(bo, bo)
        for i, g in enumerate((gq_sum[0:128, 0:128], gq_sum[128:256, 128:256], go_sum)):
            gram[i] = g if first else gram[i] + g

    grams(range(0, 1), first=True)

    def to_peer(src, dst, send, recv, off):
        remote(src, dst, send, recv, {"fs": blk(*off)}).start()

    for off in OTHERS:
        to_peer(psend.at[blk(*off)], precv.at[f], rsend, rrecv, off)
    weights.step(10)
    grams(range(1, FS))
    precv[f] = psend[f]
    loaded(mean, 8)
    loaded(square, 9)
    slab = pl.ds(pl.multiple_of((f // 2) * 128, 128), 128)
    turned[0] = mean[:, slab].T
    turned[1] = square[:, slab].T
    weights.step(11)
    peers = pl.ds(0, FS - 1)
    received(precv.at[peers], rrecv)
    total = precv[0].astype(f32)
    for j in range(1, FS):
        total += precv[j].astype(f32)
    total = total.astype(bf16)
    pall[f] = total

    def moments(p, mean_old, square_old):
        one = beta_first * mean_old + (1.0 - beta_first) * p
        two = beta_second * square_old + (1.0 - beta_second) * p * p
        return one, two, one / jnp.sqrt(two)

    own = pl.ds(pl.multiple_of(lax.rem(f, 2) * COLS, COLS), COLS)
    _, _, own_d = moments(total.astype(f32), turned[0, own, :], turned[1, own, :])
    gd = jnp.dot(
        own_d, gram[jnp.minimum(f // 4, 2)], precision=HIGH, preferred_element_type=f32
    )
    sqf[f] = jnp.broadcast_to(jnp.sum(own_d * gd, keepdims=True), (1, 128))
    for off in OTHERS:
        to_peer(sqf.at[f], sqf.at[f], fsend, frecv, off)
    for off in NEAR + ACROSS:
        to_peer(pall.at[f], pall.at[f], asend, arecv.at[0], off)
    weights.step(12)
    weights.step(13)
    received(sqf.at[peers], frecv)
    squares = sqf[0]
    for j in range(1, FS):
        squares += sqf[j]
    sqs[t] = squares

    for r in range(1, TP):
        remote(sqs.at[t], sqs.at[t], ssend, srecv, {"tp": lax.rem(t + r, TP)}).start()
    received(pall.at[pl.ds(0, len(NEAR + ACROSS))], arecv.at[0])
    upper, lower = pl.ds(0, COLS // 2), pl.ds(COLS // 2, COLS // 2)
    for step in (1, -1, 2):
        for to in (1, -1, 2):
            ref = pall.at[blk(0, step), upper, :]
            to_peer(ref, ref, asend, arecv.at[1], (to, 0))
            ref = pall.at[blk(step, 0), lower, :]
            to_peer(ref, ref, asend, arecv.at[1], (0, to))
    weights.step(14)
    received(pall.at[pl.ds(0, len(DIAGONAL + FAR))], arecv.at[1])
    firsts = [(f1q, 0), (f1q, 128), (f1v, 0), (f1v, 128)] + [(f1o, 128 * i) for i in range(4)]
    seconds = [(f2q, 0), (f2q, 128), (f2v, 0), (f2v, 128)] + [(f2o, 128 * i) for i in range(4)]
    for k in range(8):
        at = slice(128 * k, 128 * k + 128)
        p = jnp.concatenate([pall[2 * k], pall[2 * k + 1]], axis=0).astype(f32).T
        one, two, d[:, at] = moments(p, mean[:, at], square[:, at])
        ref, lo = firsts[k]
        ref[:, lo : lo + 128] = one
        ref, lo = seconds[k]
        ref[:, lo : lo + 128] = two
    hi = d[...].astype(bf16)
    lo = (d[...] - hi.astype(f32)).astype(bf16)
    bqv, bo = ball[f, 0:256, :], outputs_of(f)
    low_q = dot(bqv[:, 0:128], hi[:, 0:256]) + dot(bqv[:, 0:128], lo[:, 0:256])
    low_v = dot(bqv[:, 128:256], hi[:, 256:512]) + dot(bqv[:, 128:256], lo[:, 256:512])
    low_o = dot(bo, hi[:, 512:1024]) + dot(bo, lo[:, 512:1024])
    stq[...] = low_q
    stv[...] = low_v
    sto[...] = low_o
    received(sqs.at[pl.ds(0, TP - 1)], srecv)
    squares = sqs[0]
    for i in range(1, TP):
        squares += sqs[i]
    factor = 1.0 / jnp.sqrt(squares[0:1, 0:1] / (3.0 * MODEL * CELL) + floor_mean)
    dcopy[...] = (-learn_rate * factor * d[...]).astype(bf16)
    stq[...] = -factor * stq[...]
    stv[...] = -factor * stv[...]
    sto[...] = -factor * sto[...]
    for off in OTHERS:
        weights.block(off)
    weights.finish()
    by_core(all_sent)
    sent(psend.at[peers], rsend)
    sent(pall.at[peers], asend)
    sent(sqf.at[peers], fsend)
    sent(sqs.at[pl.ds(0, TP - 1)], ssend)


def finish_kernel(
    wall, ball, dcopy, stq, stv, sto, f1q, f1v, f1o, f2q, f2v, f2o,
    o_stq, o_stv, o_sto, o_q, o_v, o_o, o_f1q, o_f1v, o_f1o, o_f2q, o_f2v, o_f2o,
    cq, cv, co, sem, csem,
):
    plain = [
        pltpu.make_async_copy(src, dst, sem.at[i])
        for i, (src, dst) in enumerate(
            (
                (stq, o_stq), (stv, o_stv), (sto, o_sto), (f1q, o_f1q), (f1v, o_f1v),
                (f1o, o_f1o), (f2q, o_f2q), (f2v, o_f2v), (f2o, o_f2o),
            )
        )
    ]
    for cp in plain:
        cp.start()
    for k in range(FS):
        bo = jnp.concatenate([ball[k, 256:320, 0:128], ball[k, 256:320, 128:256]], axis=0)
        wq = wall[k, 0:256, 0:256].astype(f32)
        cq[k * 256 : k * 256 + 256, :] = (
            wq + dot(ball[k, 0:256, 0:128], dcopy[:, 0:256])
        ).astype(bf16)
        wv = wall[k, 0:256, 256:512].astype(f32)
        cv[k * 256 : k * 256 + 256, :] = (
            wv + dot(ball[k, 0:256, 128:256], dcopy[:, 256:512])
        ).astype(bf16)
        wo = wall[k, 256:384, :].astype(f32)
        co[k * 128 : k * 128 + 128, :] = (wo + dot(bo, dcopy[:, 512:1024])).astype(bf16)
        for i, (src, dst, n) in enumerate(((cq, o_q, 256), (cv, o_v, 256), (co, o_o, 128))):
            cp = pltpu.make_async_copy(
                src.at[pl.ds(k * n, n), :], dst.at[pl.ds(k * n, n), :], csem.at[i]
            )
            cp.start()
    for cp in plain:
        cp.wait()
    for i, (src, dst) in enumerate(((cq, o_q), (cv, o_v), (co, o_o))):
        pltpu.make_async_copy(src, dst, csem.at[i]).wait()


def local(*args):
    tokens = args[0].shape[0]
    any_spec = pl.BlockSpec(memory_space=pl.ANY)
    vmem_spec = pl.BlockSpec(memory_space=pltpu.VMEM)
    steps = [((256, 256), f32), ((256, 256), f32), ((128, 512), f32)]
    news = [((MODEL, 256), bf16), ((MODEL, 256), bf16), ((CELL, 512), bf16)]
    moment = [((128, 256), f32), ((128, 256), f32), ((128, 512), f32)]
    mids = [((FS, W_ROWS, 512), bf16), ((FS, B_ROWS, 256), bf16), ((128, 1024), bf16)]
    mids += steps + moment + moment
    outs = steps + news + moment + moment
    dma = pltpu.SemaphoreType.DMA
    mid = pl.pallas_call(
        gather_kernel,
        out_shape=[pltpu.VMEM(s, t) for s, t in mids],
        in_specs=[any_spec] * 17,
        out_specs=[vmem_spec] * len(mids),
        scratch_shapes=[
            pltpu.VMEM((tokens, MODEL), bf16),
            pltpu.VMEM((tokens, CELL), bf16),
            pltpu.VMEM((tokens, 256), bf16),
            pltpu.VMEM((tokens, 256), bf16),
            pltpu.VMEM((tokens, 512), bf16),
            pltpu.VMEM((256, 512), f32),
            pltpu.VMEM((128, 512), f32),
            pltpu.VMEM((128, 1024), f32),
            pltpu.VMEM((128, 1024), f32),
            pltpu.VMEM((tokens, 256), f32),
            pltpu.VMEM((tokens, 128), f32),
            pltpu.VMEM((1024, tokens), bf16),
            pltpu.VMEM((tokens, 768), bf16),
            pltpu.VMEM((FS, COLS, 128), bf16),
            pltpu.VMEM((FS, COLS, 128), bf16),
            pltpu.VMEM((FS, COLS, 128), bf16),
            pltpu.VMEM((3, 128, 128), f32),
            pltpu.VMEM((2, 128, 128), f32),
            pltpu.VMEM((128, 1024), f32),
            pltpu.VMEM((FS, 1, 128), f32),
            pltpu.VMEM((TP, 1, 128), f32),
            dma((10,)),
            dma, dma((STEPS,)), dma, dma((4,)), dma, dma((4,)), dma, dma((8,)),
            dma, dma, dma, dma((2,)), dma, dma, dma, dma,
            pltpu.SemaphoreType.REGULAR,
        ],
        compiler_params=pltpu.CompilerParams(
            collective_id=0, has_side_effects=True, vmem_limit_bytes=50 * 1024 * 1024
        ),
        name="gather_and_reduce",
    )(*args)
    return tuple(
        pl.pallas_call(
            finish_kernel,
            out_shape=[jax.ShapeDtypeStruct(s, t) for s, t in outs],
            in_specs=[vmem_spec] * len(mids),
            out_specs=[any_spec] * len(outs),
            scratch_shapes=[
                pltpu.VMEM((MODEL, 256), bf16),
                pltpu.VMEM((MODEL, 256), bf16),
                pltpu.VMEM((CELL, 512), bf16),
                dma((9,)),
                dma((3,)),
            ],
            compiler_params=pltpu.CompilerParams(vmem_limit_bytes=12 * 1024 * 1024),
            name="write_copies",
        )(*mid)
    )


def solution(mesh):
    fs, both, tp = P("fs", None), P("fs", "tp"), P(None, "tp")
    in_specs = (fs, fs) + (both,) * 6 + (fs,) * 3 + (tp,) * 6
    out_specs = (both,) * 3 + (tp,) * 9
    return jax.shard_map(local, mesh=mesh, in_specs=in_specs, out_specs=out_specs, check_vma=False)
```
